256 devices in a mesh: fs: 64 (over z, x, core), tp: 4 (over y).
Axes of the slice: x: 4, y: 4, z: 8, core: 2. Of those that a mesh axis runs over, the one named last changes fastest.
Arguments:
- tokens: bfloat16 [768, 4, 2048], P(None, 'tp'), may hold values from -6 to 6
- norm_gain: float32 [2048], P('fs'), may hold values from 0.1 to 1.9
- gate_weight: float32 [8, 2048, 4096], P(None, 'fs', 'tp'), may hold values from -0.125 to 0.125
- up_weight: float32 [8, 2048, 4096], P(None, 'fs', 'tp'), may hold values from -0.125 to 0.125
- down_weight: float32 [8, 2048, 4096], P(None, 'fs', 'tp'), may hold values from -0.09375 to 0.09375
- expert_ids: int32 [768, 4, 2], P(None, 'tp'), may hold values from 0 to 7, all different within a row
- expert_mix: float32 [768, 4, 2], P(None, 'tp'), may hold values from 0.2 to 1
Outputs:
- gate_serve: bfloat16 [8, 2048, 4096], P(None, None, 'fs')
- up_serve: bfloat16 [8, 2048, 4096], P(None, None, 'fs')
- down_serve: bfloat16 [8, 2048, 4096], P(None, None, 'fs')
- mixed: bfloat16 [768, 4, 2048], P('fs', 'tp')
The draws below stay inside these ranges and needn't reach their ends.
Inputs may be any that keep to these rules, and one draw needn't show every extreme that they name: `expert_ids`: each token names two different experts.
All inputs are finite; a program needn't handle non-finite values.
Results may differ from the reference program's by a relative error of at most 0.0082.
Values may be sent and summed in bfloat16 or wider, within the bound.
A program may use at most 64 MiB of HBM per device.

```python
import jax
import jax.numpy as jnp
from jax import lax

D = 2048
FF = 4096
EXPERTS = 8
ROWS = 768
N_TP = 4


def shard_levels(rng, shape, pieces, smallest, top_value):
    gain, own = 1.0, jax.random.fold_in(rng, 6)
    for axis_at, parts in pieces:
        heights = jnp.exp(jax.random.uniform(jax.random.fold_in(own, axis_at), (parts,), jnp.float32, smallest / len(pieces), top_value / len(pieces)))
        gain = gain * jnp.repeat(heights, shape[axis_at] // parts).reshape([-1 if axis == axis_at else 1 for axis in range(len(shape))])
    return gain


def picks_of(key, rows, count, top, lift):
    order = jax.random.permutation(jax.random.fold_in(key, 1), count)
    pull = order
    for power in range(3):
        pull = pull * pull // count
    pull = pull * lift // count
    tickets = jax.random.randint(jax.random.fold_in(key, 2), (rows, count), 0, 4096) + pull
    fixed_rows = jax.random.permutation(jax.random.fold_in(key, 3), rows)[jnp.arange(count) % rows]
    tickets = jnp.where(jnp.arange(rows)[:, None] == fixed_rows[None, :], 1 << 14, tickets)
    priority = tickets * count + jnp.arange(count)
    return lax.top_k(priority.astype(jnp.int32), top)[1].astype(jnp.int32)


def normal_values(rng, dims, deviation, reach, pieces=(), held_as=jnp.bfloat16):
    entries = jax.random.normal(rng, dims, jnp.float32) * deviation
    if len(pieces) > 0:
        entries = shard_levels(rng, dims, pieces, -0.22, 0.18) * entries
    return jnp.clip(entries, min=-reach, max=reach).astype(held_as)


def setup_inputs(seed: int = 0) -> dict:
    key_of = jax.random.split(jax.random.key(seed), 8)
    tokens = normal_values(key_of[0], (ROWS, N_TP, D), 1.0, 6.0, ((1, 4),))
    norm_gain = jnp.clip(1.0 + 0.18 * jax.random.normal(key_of[1], (D,), jnp.float32), 0.1, 1.9)
    gate_weight = normal_values(key_of[2], (EXPERTS, D, FF), D ** -0.5, 0.125, ((1, 64), (2, 4)), jnp.float32)
    up_weight = normal_values(key_of[3], (EXPERTS, D, FF), D ** -0.5, 0.125, ((1, 64), (2, 4)), jnp.float32)
    down_weight = normal_values(key_of[4], (EXPERTS, D, FF), FF ** -0.5, 0.09375, ((1, 64), (2, 4)), jnp.float32)
    expert_ids = picks_of(key_of[5], ROWS * N_TP, EXPERTS, 2, 0).reshape((ROWS, N_TP, 2))
    expert_mix = jnp.clip(0.2 + 0.8 * jax.random.uniform(key_of[6], (ROWS, N_TP, 2), jnp.float32) ** shard_levels(key_of[6], (ROWS, N_TP, 2), ((1, 4),), -0.2, 0.2), 0.2, 1.0)
    return dict(tokens=tokens, norm_gain=norm_gain, gate_weight=gate_weight, up_weight=up_weight, down_weight=down_weight, expert_ids=expert_ids, expert_mix=expert_mix)


norm_eps = 1e-05

def reference(tokens, norm_gain, gate_weight, up_weight, down_weight, expert_ids, expert_mix):
    gate_serve = (gate_weight * norm_gain[None, :, None]).astype(jnp.bfloat16)
    up_serve = (up_weight * norm_gain[None, :, None]).astype(jnp.bfloat16)
    down_serve = down_weight.astype(jnp.bfloat16)
    token_rows = tokens.reshape(-1, D).astype(jnp.float32)
    row_mean = lax.optimization_barrier(jnp.mean(token_rows, axis=1, keepdims=True))
    centered = token_rows - row_mean
    variance = lax.optimization_barrier(jnp.mean(centered * centered, axis=1, keepdims=True))
    normed = (centered * lax.rsqrt(variance + norm_eps)).astype(jnp.bfloat16)
    route_ids = expert_ids.reshape(-1, 2)
    route_mix = expert_mix.reshape(-1, 2)
    expert_iota = jnp.arange(EXPERTS, dtype=jnp.int32)
    expert_gates = lax.optimization_barrier(jnp.sum((route_ids[:, :, None] == expert_iota[None, None, :]).astype(jnp.float32) * route_mix[:, :, None], axis=1))

    def add_expert(running, weights_now):
        gate_mat, up_mat, down_mat, gate_col = weights_now
        gate_act = jnp.dot(normed, gate_mat, preferred_element_type=jnp.float32)
        up_act = jnp.dot(normed, up_mat, preferred_element_type=jnp.float32)
        hidden = (jax.nn.silu(gate_act) * up_act * gate_col[:, None]).astype(jnp.bfloat16)
        product = lax.dot_general(hidden, down_mat, (((1,), (1,)), ((), ())), preferred_element_type=jnp.float32)
        return (running + product, None)
    start_sum = jnp.zeros((token_rows.shape[0], D), jnp.float32)
    summed, _ = lax.scan(add_expert, start_sum, (gate_serve, up_serve, down_serve, expert_gates.T))
    mixed = summed.astype(jnp.bfloat16).reshape(ROWS, N_TP, D)
    return (gate_serve, up_serve, down_serve, mixed)
```

```python
import functools

import jax
import jax.numpy as jnp
from jax import lax
from jax.experimental import pallas as pl
from jax.experimental.pallas import tpu as pltpu
from jax.sharding import PartitionSpec as P

norm_eps = 1e-05
MESH = pl.DeviceIdType.MESH
BF16, F32 = jnp.bfloat16, jnp.float32
NZ, NX, NC = 8, 4, 2


def pack_kernel(gate, up, down, gain, pg, pd):
    lanes = lax.broadcasted_iota(jnp.int32, (32, 128), 1)
    low = lanes < 64
    scale = gain[...]

    def pair(ref, j, scaled):
        a, b = (ref[e, :, 128 * j:128 * (j + 1)] for e in range(2))
        if scaled:
            a, b = a * scale, b * scale
        even = jnp.where(low, a, pltpu.roll(b, 64, 1))
        odd = jnp.where(low, pltpu.roll(a, 64, 1), b)
        return even.astype(BF16), odd.astype(BF16)

    for j in range(8):
        for s, ref in ((0, gate), (1, up)):
            for o, v in enumerate(pair(ref, j, True)):
                for half in range(2):
                    pg[half, 0, 2 * j + o, :, 128 * s:128 * (s + 1)] = v[16 * half:16 * (half + 1)]
        for o, v in enumerate(pair(down, j, False)):
            pd[0, 2 * j + o] = v


def pack(gate_weight, up_weight, down_weight, gain):
    block = pl.BlockSpec((2, 32, 1024), lambda q: (q, 0, 0))
    return pl.pallas_call(
        pack_kernel,
        grid=(4,),
        in_specs=[block, block, block, pl.BlockSpec((32, 1), lambda q: (0, 0))],
        out_specs=[
            pl.BlockSpec((2, 1, 16, 16, 256), lambda q: (0, q, 0, 0, 0)),
            pl.BlockSpec((1, 16, 32, 128), lambda q: (q, 0, 0, 0)),
        ],
        out_shape=(
            jax.ShapeDtypeStruct((2, 4, 16, 16, 256), BF16),
            jax.ShapeDtypeStruct((4, 16, 32, 128), BF16),
        ),
        cost_estimate=pl.CostEstimate(flops=2000000, bytes_accessed=5 * 2**20, transcendentals=0),
    )(gate_weight, up_weight, down_weight, gain)


def main_kernel(pg, pd, tok, gates, wg_out, dn_out, mixed, lg, ld, wg, dn, tokv, normed, hid, part, own, core_land,
                xs, x_land, zs, z_land, fin, fin_land, s1_send, s1_recv, s2_send, s2_recv, ag_send, ag_recv,
                core_send, core_recv, x_send, x_recv, z_send, z_recv, fin_send, fin_recv, tok_sem, out_sem):
    f, t = lax.axis_index("fs"), lax.axis_index("tp")
    z, x, c = lax.div(f, NX * NC), lax.rem(lax.div(f, NC), NX), lax.rem(f, NC)
    mate = f + 1 - 2 * c
    right, left, far = lax.rem(t + 1, 4), lax.rem(t + 3, 4), lax.rem(t + 2, 4)

    def remote(src, dst, send, recv, device):
        return pltpu.make_async_remote_copy(
            src_ref=src, dst_ref=dst, send_sem=send, recv_sem=recv, device_id=device, device_id_type=MESH)

    def s1(k, d):
        q = lax.rem(t + d, 4)
        sems = (s1_send.at[k, d - 1], s1_recv.at[k, d - 1], (f, q))
        if k < 2:
            return remote(pg.at[k, q], lg.at[k, pl.ds(16 * t, 16)], *sems)
        return remote(pd.at[q], ld.at[pl.ds(16 * t, 16)], *sems)

    def s2_send_all(k):
        def some(m, carry):
            for zi in range(NZ):
                zo = (zi + 1) // 2 if zi % 2 else NZ - zi // 2
                zd = lax.rem(z + zo, NZ)
                xd = lax.rem(x + lax.rem(m + zi, NX), NX)
                cd = lax.rem(c + lax.div(m, NX), NC)
                u = zd * (NX * NC) + xd * NC + cd
                sems = (s2_send.at[k], s2_recv.at[k], (u, t))

                def go():
                    if k < 2:
                        remote(lg.at[k, u], wg.at[t, f, k], *sems).start()
                    else:
                        remote(ld.at[u], dn.at[t, f], *sems).start()

                if zi == 0:
                    pl.when(m > 0)(go)
                else:
                    go()
            return carry

        lax.fori_loop(0, NZ, some, 0)
        if k < 2:
            wg[t, f, k] = lg[k, f]
        else:
            dn[t, f] = ld[f]

    def s2_all(k):
        others = pl.ds(0, NZ * NX * NC - 1)
        sems = (s2_send.at[k], s2_recv.at[k], (mate, t))
        if k < 2:
            return remote(lg.at[k, others], wg.at[t, others, k], *sems)
        return remote(ld.at[others], dn.at[t, others], *sems)

    def ag_piece(k, q, piece):
        if k < 2:
            return wg.at[q, pl.ds(32 * piece, 32), k]
        return dn.at[q, pl.ds(16 * (k - 2) + 8 * piece, 8)]

    def ag(k, slot, arriving=False):
        piece = (0, 1, 0, 1, 0, 1)[slot]
        to = (right, right, left, left, right, left)[slot]
        if arriving:
            q = (left, left, right, right, far, far)[slot]
        else:
            q = (t, t, t, t, left, right)[slot]
        ref = ag_piece(k, q, piece)
        return remote(ref, ref, ag_send.at[k, slot], ag_recv.at[k, slot], (f, to))

    def ag_own(k):
        for slot in (0, 3, 1, 2):
            ag(k, slot).start()

    def ag_wait(k, slot):
        ag(k, slot, True).wait_recv()

    def ag_forward(k):
        ag_wait(k, 0)
        ag(k, 4).start()
        ag_wait(k, 3)
        ag(k, 5).start()

    def tok_copy(i):
        return pltpu.make_async_copy(tok.at[:, i], tokv.at[i], tok_sem.at[i])

    def norm(i):
        tok_copy(i).wait()

        def two(a, carry):
            v = jnp.concatenate([tokv[i, 2 * a].astype(F32), tokv[i, 2 * a + 1].astype(F32)], axis=0)
            mean = jnp.mean(v, axis=1, keepdims=True)
            v = v - mean
            var = jnp.mean(v * v, axis=1, keepdims=True)
            rows = pl.ds(pl.multiple_of(192 * i + 48 * a, 16), 48)
            normed[rows, :] = (v * lax.rsqrt(var + norm_eps)).astype(BF16)
            return carry

        lax.fori_loop(0, NZ // 2, two, 0)

    def hidden(q):
        def some(r, carry):
            rows = pl.ds(pl.multiple_of(r * 256, 256), 256)
            act = jnp.dot(normed[rows, :], wg[q].reshape(2048, 256), preferred_element_type=F32)
            gate_act, up_act = act[:, :128], act[:, 128:]
            value = gate_act / (1.0 + jnp.exp(-gate_act)) * up_act * gates[q, rows, :]
            hid[q, rows, :] = value.astype(BF16)
            return carry

        lax.fori_loop(0, 3, some, 0)

    def out_copy(q, which):
        if which == 0:
            return pltpu.make_async_copy(wg.at[q], wg_out.at[q], out_sem.at[q, 0])
        return pltpu.make_async_copy(dn.at[q], dn_out.at[q], out_sem.at[q, 1])

    def core_copy(j):
        return remote(part.at[j], core_land.at[j], core_send.at[j], core_recv.at[j], (mate, t))

    def x_copy(j, d):
        xd = lax.rem(x + d, NX)
        return remote(xs.at[j, xd], x_land.at[j, d - 1], x_send.at[j, d - 1], x_recv.at[j, d - 1],
                      (z * (NX * NC) + xd * NC + c, t))

    def z_copy(j, d):
        zd = lax.rem(z + d, NZ)
        return remote(zs.at[j, zd], z_land.at[j, d - 1], z_send.at[j, d - 1], z_recv.at[j, d - 1],
                      (zd * (NX * NC) + x * NC + c, t))

    def fin_copy(j):
        return remote(fin.at[j], fin_land.at[j], fin_send.at[j], fin_recv.at[j], (mate, t))

    def down_half(j, side, r):
        rows = pl.ds(pl.multiple_of(r * 256, 256), 256)
        total = jnp.zeros((256, 256), F32)
        for q in range(4):
            block = dn[q, pl.ds(16 * j + 8 * side, 8)].reshape(256, 128)
            total += lax.dot_general(hid[q, rows, :], block, (((1,), (1,)), ((), ())), preferred_element_type=F32)
        return rows, total

    def step_a(j):
        k = j + 2
        ag_forward(k)
        if j + 2 < 4:
            ag_own(k + 2)
        for slot in (1, 2, 4, 5):
            ag_wait(k, slot)

        def for_mate(r, carry):
            rows, total = down_half(j, 1 - c, r)
            part[j, rows, :] = total.astype(BF16)
            return carry

        def for_own(r, carry):
            rows, total = down_half(j, c, r)
            own[rows, :] = total
            return carry

        lax.fori_loop(0, 3, for_mate, 0)
        core_copy(j).start()
        lax.fori_loop(0, 3, for_own, 0)

    def step_b(j):
        core_copy(j).wait_recv()
        for i in range(NX):
            rows = slice(192 * i, 192 * (i + 1))
            xs[j, i] = (own[rows, :] + core_land[j, rows, :].astype(F32)).astype(BF16)
        for d in (2, 1, 3):
            x_copy(j, d).start()

    def step_c(j):
        for d in (1, 2, 3):
            x_copy(j, d).wait_recv()
        total = xs[j, x].astype(F32)
        for d in range(3):
            total += x_land[j, d].astype(F32)
        zs[j] = total.reshape(NZ, 24, 256).astype(BF16)
        for d in (4, 3, 5, 2, 6, 1, 7):
            z_copy(j, d).start()

    def step_d(j):
        for d in range(1, NZ):
            z_copy(j, d).wait_recv()
        total = zs[j, z].astype(F32)
        for d in range(NZ - 1):
            total += z_land[j, d].astype(F32)
        fin[j] = total.astype(BF16)
        fin_copy(j).start()

    def step_e(j):
        fin_copy(j).wait_recv()
        for side, ref in ((c, fin), (1 - c, fin_land)):
            value = ref[j].astype(F32)
            rows = jnp.where(c == 0, value[:12], value[12:])
            mixed[:, pl.ds(pl.multiple_of(512 * j + 256 * side, 256), 256)] = rows.astype(BF16)

    for i in range(NX):
        tok_copy(i).start()
    for k in range(3):
        for d in (2, 1, 3):
            s1(k, d).start()
    for k in range(2):
        lg[k, pl.ds(16 * t, 16)] = pg[k, t]
    ld[pl.ds(16 * t, 16)] = pd[t]

    for k in range(3):
        for d in (1, 3, 2):
            s1(k, d).wait_recv()
        s2_send_all(k)
        if k < 2:
            norm(2 * k)
            norm(2 * k + 1)
    s2_all(0).wait_recv()
    ag_own(0)
    s2_all(1).wait_recv()
    ag_own(1)
    ag_forward(0)
    out_copy(t, 0).start()
    hidden(t)
    s2_all(2).wait_recv()
    out_copy(t, 1).start()
    ag_forward(1)
    ag_own(2)
    ag_own(3)
    for k in range(2):
        for slot in (1, 2):
            ag_wait(k, slot)
    out_copy(left, 0).start()
    out_copy(right, 0).start()
    hidden(left)
    hidden(right)
    for k in range(2):
        for slot in (4, 5):
            ag_wait(k, slot)
    out_copy(far, 0).start()
    hidden(far)
    step_a(0)
    step_b(0)
    step_a(1)
    step_c(0)
    step_b(1)
    step_a(2)
    step_d(0)
    step_c(1)
    step_b(2)
    step_a(3)
    for q in (left, right, far):
        out_copy(q, 1).start()
    step_d(1)
    step_c(2)
    step_b(3)
    step_d(2)
    step_c(3)
    step_d(3)
    for j in range(4):
        step_e(j)

    for k in range(3):
        for d in (1, 2, 3):
            s1(k, d).wait_send()
        s2_all(k).wait_send()
    for k in range(6):
        for slot in range(6):
            ag(k, slot).wait_send()
    for j in range(4):
        core_copy(j).wait_send()
        fin_copy(j).wait_send()
        for d in range(1, NX):
            x_copy(j, d).wait_send()
        for d in range(1, NZ):
            z_copy(j, d).wait_send()
    for q in range(4):
        for which in range(2):
            out_copy(q, which).wait()


def exchange(pg, pd, tok, gates):
    dma, vmem = pltpu.SemaphoreType.DMA, pltpu.VMEM
    whole = pl.BlockSpec(memory_space=pltpu.VMEM)
    anywhere = pl.BlockSpec(memory_space=pl.ANY)
    return pl.pallas_call(
        main_kernel,
        in_specs=[whole, whole, anywhere, whole],
        out_specs=[anywhere, anywhere, whole],
        out_shape=(
            jax.ShapeDtypeStruct((4, 64, 2, 16, 256), BF16),
            jax.ShapeDtypeStruct((4, 64, 32, 128), BF16),
            jax.ShapeDtypeStruct((12, 2048), BF16),
        ),
        scratch_shapes=[
            vmem((2, 64, 16, 256), BF16),
            vmem((64, 32, 128), BF16),
            vmem((4, 64, 2, 16, 256), BF16),
            vmem((4, 64, 32, 128), BF16),
            vmem((NX, NZ, 24, 2048), BF16),
            vmem((768, 2048), BF16),
            vmem((4, 768, 128), BF16),
            vmem((4, 768, 256), BF16),
            vmem((768, 256), F32),
            vmem((4, 768, 256), BF16),
            vmem((4, NX, 192, 256), BF16),
            vmem((4, NX - 1, 192, 256), BF16),
            vmem((4, NZ, 24, 256), BF16),
            vmem((4, NZ - 1, 24, 256), BF16),
            vmem((4, 24, 256), BF16),
            vmem((4, 24, 256), BF16),
            dma((3, 3)), dma((3, 3)),
            dma((3,)), dma((3,)),
            dma((6, 6)), dma((6, 6)),
            dma((4,)), dma((4,)),
            dma((4, 3)), dma((4, 3)),
            dma((4, 7)), dma((4, 7)),
            dma((4,)), dma((4,)),
            dma((4,)), dma((4, 2)),
        ],
        compiler_params=pltpu.CompilerParams(has_side_effects=True, vmem_limit_bytes=56 * 2**20),
    )(pg, pd, tok, gates)


def turn_kernel(wg, dn, gate_out, up_out, down_out):
    both = wg[0]
    for out, value in ((gate_out, both[:, :128]), (up_out, both[:, 128:]), (down_out, dn[0])):
        out[...] = value.T.reshape(2, 64, value.shape[0])


def turned(wg, dn):
    out = pl.BlockSpec((2, 64, 1024), lambda q, d: (q, 0, d))
    shape = jax.ShapeDtypeStruct((8, 64, 2048), BF16)
    return pl.pallas_call(
        turn_kernel,
        grid=(4, 2),
        in_specs=[pl.BlockSpec((1, 1024, 256), lambda q, d: (q, d, 0)),
                  pl.BlockSpec((1, 1024, 128), lambda q, d: (q, d, 0))],
        out_specs=[out] * 3,
        out_shape=(shape,) * 3,
        cost_estimate=pl.CostEstimate(flops=2000000, bytes_accessed=12 * 2**20, transcendentals=0),
    )(wg.reshape(4, 2048, 256), dn.reshape(4, 2048, 128))


def local(tokens, norm_gain, gate_weight, up_weight, down_weight, expert_ids, expert_mix):
    pg, pd = pack(gate_weight, up_weight, down_weight, norm_gain[:, None])
    tok = tokens.reshape(NZ, NX, 24, 2048)
    order = lambda a: a.reshape(NZ, NX, 24, 2).transpose(1, 0, 2, 3).reshape(768, 2)
    ids, mix = order(expert_ids), order(expert_mix)
    expert = 2 * jnp.arange(4, dtype=jnp.int32)[:, None] + (jnp.arange(128, dtype=jnp.int32) // 64)[None, :]
    gates = sum(jnp.where(ids[None, :, k, None] == expert[:, None, :], mix[None, :, k, None], 0.0) for k in range(2))
    wg, dn, mixed = exchange(pg, pd, tok, gates)
    outs = tuple(jnp.swapaxes(out, 1, 2) for out in turned(wg, dn))
    return outs + (mixed.reshape(12, 1, 2048),)


def solution(mesh):
    return jax.shard_map(
        local,
        mesh=mesh,
        in_specs=(
            P(None, "tp", None),
            P("fs"),
            P(None, "fs", "tp"),
            P(None, "fs", "tp"),
            P(None, "fs", "tp"),
            P(None, "tp", None),
            P(None, "tp", None),
        ),
        out_specs=(
            P(None, None, "fs"),
            P(None, None, "fs"),
            P(None, None, "fs"),
            P("fs", "tp", None),
        ),
        check_vma=False,
    )
```

```python
import functools

import jax
import jax.numpy as jnp
from jax import lax
from jax.experimental import pallas as pl
from jax.experimental.pallas import tpu as pltpu
from jax.sharding import PartitionSpec as P

norm_eps = 1e-05
MESH = pl.DeviceIdType.MESH
BF16, F32 = jnp.bfloat16, jnp.float32
NZ, NX, NC = 8, 4, 2


ALL = NZ * NX * NC
LANES = (slice(0, 128), slice(128, 256), slice(0, 256))
HALF = (0, 0, 1)
DOWN = tuple((8 * j, 8) for j in range(8))
AHEAD = 3


def order_of_steps():
    when, y, x, z = [], 0.0, 0.0, 0.0
    for j, (_, count) in enumerate(DOWN):
        y += count / 8
        x = max(x, y + 0.9) + count / 8
        z = max(z, x + 1.4) + count / 16
        when += [(y - 2.8, 0, "F", j), (y, 1, "a", j), (y + 0.9, 2, "b", j), (x + 1.4, 3, "c", j), (z + 1.9, 4, "d", j)]
    return [(step, j) for _, _, step, j in sorted(when)]


def main_kernel(gate_in, up_in, down_in, gain_in, tok, ids_in, mix_in, gate_out, up_out, down_out, mixed,
                raw, gainv, idsv, mixv, gates, pg, pd, lg, ld, wg, dn, tokv, normed, hid, part, own, core_land,
                xs, x_land, zs, z_land, s1_send, s1_recv, s2_send, s2_recv, ag_send, ag_recv,
                core_send, core_recv, x_send, x_recv, z_send, z_recv, in_sem):
    f, t = lax.axis_index("fs"), lax.axis_index("tp")
    z, x, c = lax.div(f, NX * NC), lax.rem(lax.div(f, NC), NX), lax.rem(f, NC)
    mate = f + 1 - 2 * c
    right, left, far = lax.rem(t + 1, 4), lax.rem(t + 3, 4), lax.rem(t + 2, 4)

    def remote(src, dst, send, recv, device):
        return pltpu.make_async_remote_copy(
            src_ref=src, dst_ref=dst, send_sem=send, recv_sem=recv, device_id=device, device_id_type=MESH)

    def others(act):
        def some(m, carry):
            for zi in range(NZ):
                zo = (zi + 1) // 2 if zi % 2 else NZ - zi // 2
                zd = lax.rem(z + zo, NZ)
                xd = lax.rem(x + lax.rem(m + zi, NX), NX)
                cd = lax.rem(c + lax.div(m, NX), NC)
                u = zd * (NX * NC) + xd * NC + cd
                if zi == 0:
                    pl.when(m > 0)(functools.partial(act, u))
                else:
                    act(u)
            return carry

        lax.fori_loop(0, NZ, some, 0)

    def enter():
        barrier = pltpu.get_barrier_semaphore()

        def greet(device):
            pl.semaphore_signal(barrier, inc=1, device_id=device, device_id_type=MESH)

        near = [lax.rem(x + xo, NX) * NC + lax.rem(c + co, NC) for xo in (2, 1, 3, 0) for co in range(NC)]
        for zo in (4, 3, 5, 2, 6, 1, 7, 0):
            base = lax.rem(z + zo, NZ) * (NX * NC)
            for n, u in enumerate(near):
                if zo or n != 2 * NX - 2:
                    greet((base + u, t))
        for d in (2, 1, 3):
            greet((f, lax.rem(t + d, 4)))
        return barrier

    def raw_copy(i):
        return pltpu.make_async_copy((gate_in, up_in, down_in)[i], raw.at[i], in_sem.at[i])

    def small_copy(i):
        src, dst = ((gain_in, gainv), (ids_in, idsv), (mix_in, mixv))[i]
        return pltpu.make_async_copy(src, dst, in_sem.at[3 + i])

    def tok_copy(i):
        return pltpu.make_async_copy(tok.at[:, i], tokv.at[i], in_sem.at[6 + i])

    def pack(i):
        low = lax.broadcasted_iota(jnp.int32, (32, 128), 1) < 64
        square = [lax.broadcasted_iota(jnp.int32, (32, 32), axis) for axis in (0, 1)]
        spread = jnp.where(square[0] == square[1], jnp.broadcast_to(gainv[...], (32, 32)), 0.0)
        scale = jnp.sum(spread, axis=1, keepdims=True)
        raw_copy(i).wait()

        def some(q, carry):
            for j in range(8):
                a, b = (raw[i, 2 * q + e, :, 128 * j:128 * (j + 1)] for e in range(2))
                if i < 2:
                    a, b = a * scale, b * scale
                even = jnp.where(low, a, pltpu.roll(b, 64, 1)).astype(BF16)
                odd = jnp.where(low, pltpu.roll(a, 64, 1), b).astype(BF16)
                for o, v in enumerate((even, odd)):
                    if i < 2:
                        for half in range(2):
                            pg[half, q, 2 * j + o, :, 128 * i:128 * (i + 1)] = v[16 * half:16 * (half + 1)]
                    else:
                        pd[q, 2 * j + o] = v
            return carry

        lax.fori_loop(0, 4, some, 0)
        if i < 2:
            for half in range(2):
                lanes = slice(128 * i, 128 * (i + 1))
                lg[half, pl.ds(16 * t, 16), :, lanes] = pg[half, t, :, :, lanes]
        else:
            ld[pl.ds(16 * t, 16)] = pd[t]

    def spread_gates():
        small_copy(1).wait()
        small_copy(2).wait()
        for q in range(4):
            sides = []
            for e in (2 * q, 2 * q + 1):
                row = sum(jnp.where(idsv[k:k + 1, :] == e, mixv[k:k + 1, :], 0.0) for k in range(2))
                sides.append(jnp.broadcast_to(row, (64, 768)))
            turned = jnp.concatenate(sides, axis=0).T
            for ci in range(NC):
                for xi in range(NX):
                    for zi in range(NZ):
                        at, by = 384 * ci + 96 * xi + 12 * zi, 96 * zi + 24 * xi + 12 * ci
                        gates[q, at:at + 12, :] = turned[by:by + 12, :]

    def s1(k, d):
        q = lax.rem(t + d, 4)
        sems = (s1_send.at[k], s1_recv.at[k], (f, q))
        if k < 3:
            return remote(pg.at[HALF[k], q, :, :, LANES[k]], lg.at[HALF[k], pl.ds(16 * t, 16), :, LANES[k]], *sems)
        return remote(pd.at[q], ld.at[pl.ds(16 * t, 16)], *sems)

    def s1_start(k):
        for d in (2, 1, 3):
            s1(k, d).start()

    def s1_all(k):
        sems = (s1_send.at[k], s1_recv.at[k], (f, right))
        if k < 3:
            return remote(pg.at[HALF[k], pl.ds(0, 3), :, :, LANES[k]], pg.at[HALF[k], pl.ds(0, 3), :, :, LANES[k]], *sems)
        return remote(pd.at[pl.ds(0, 3)], pd.at[pl.ds(0, 3)], *sems)

    def s1_wait(k):
        s1_all(k).wait_recv()

    def s2_send_all(k):
        def go(u):
            sems = (s2_send.at[k], s2_recv.at[k], (u, t))
            if k < 3:
                remote(lg.at[HALF[k], u, :, LANES[k]], wg.at[t, f, HALF[k], :, LANES[k]], *sems).start()
            else:
                remote(ld.at[u], dn.at[t, f], *sems).start()

        others(go)
        if k < 3:
            wg[t, f, HALF[k], :, LANES[k]] = lg[HALF[k], f, :, LANES[k]]
        else:
            dn[t, f] = ld[f]

    def s2_all(k):
        blocks = pl.ds(0, ALL - 1)
        sems = (s2_send.at[k], s2_recv.at[k], (mate, t))
        if k < 3:
            return remote(lg.at[HALF[k], blocks, :, LANES[k]], wg.at[t, blocks, HALF[k], :, LANES[k]], *sems)
        return remote(ld.at[blocks], dn.at[t, blocks], *sems)

    def ag_piece(k, q, piece):
        if k < 3:
            return wg.at[q, pl.ds(32 * piece, 32), HALF[k], :, LANES[k]]
        first, count = DOWN[k - 3]
        return dn.at[q, pl.ds(first + count // 2 * piece, count // 2)]

    def ag(k, slot):
        piece = (0, 1, 0, 1, 0, 1)[slot]
        to = (right, right, left, left, right, left)[slot]
        q = (t, t, t, t, left, right)[slot]
        ref = ag_piece(k, q, piece)
        return remote(ref, ref, ag_send.at[k], ag_recv.at[k, (0, 2, 2, 1, 3, 3)[slot]], (f, to))

    def ag_own(k):
        for slot in (0, 3, 1, 2):
            ag(k, slot).start()

    def ag_arrived(k, group):
        if group < 2:
            ref = ag_piece(k, (left, right)[group], group)
        elif k < 3:
            ref = wg.at[far, :, HALF[k], :, LANES[k]]
        else:
            ref = dn.at[far, pl.ds(*DOWN[k - 3])]
        remote(ref, ref, ag_send.at[k], ag_recv.at[k, group], (f, right)).wait_recv()

    def ag_sent(k):
        if k < 3:
            ref = wg.at[pl.ds(0, 3), :, HALF[k], :, LANES[k]]
        else:
            ref = dn.at[pl.ds(0, 3), pl.ds(*DOWN[k - 3])]
        remote(ref, ref, ag_send.at[k], ag_recv.at[k, 0], (f, right)).wait_send()

    def ag_forward(k):
        ag_arrived(k, 0)
        ag(k, 4).start()
        ag_arrived(k, 1)
        ag(k, 5).start()

    def norm(i):
        tok_copy(i).wait()

        def four(a, carry):
            v = jnp.concatenate([tokv[i, 4 * a + b].astype(F32) for b in range(4)], axis=0)
            mean = jnp.mean(v, axis=1, keepdims=True)
            v = v - mean
            var = jnp.mean(v * v, axis=1, keepdims=True)
            v = v * lax.rsqrt(var + norm_eps)
            for ci in range(NC):
                some = jnp.concatenate([v[24 * b + 12 * ci:24 * b + 12 * (ci + 1)] for b in range(4)], axis=0)
                rows = pl.ds(pl.multiple_of(384 * ci + 96 * i + 48 * a, 16), 48)
                normed[rows, :] = some.astype(BF16)
            return carry

        lax.fori_loop(0, NZ // 4, four, 0)

    def hidden(q):
        def some(r, carry):
            rows = pl.ds(pl.multiple_of(r * 256, 256), 256)
            act = jnp.dot(normed[rows, :], wg[q].reshape(2048, 256), preferred_element_type=F32)
            gate_act, up_act = act[:, :128], act[:, 128:]
            value = gate_act / (1.0 + jnp.exp(-gate_act)) * up_act * gates[q, rows, :]
            hid[rows, pl.ds(pl.multiple_of(q * 128, 128), 128)] = value.astype(BF16)
            return carry

        lax.fori_loop(0, 3, some, 0)

    def turn_both(q):
        for i in range(4):
            both = wg[q, 16 * i:16 * (i + 1)].reshape(512, 256).T
            for n, out in enumerate((gate_out, up_out)):
                for e in range(2):
                    out[2 * q + e, :, 512 * i:512 * (i + 1)] = both[128 * n + 64 * e:128 * n + 64 * (e + 1), :]

    def turn_down(q, i):
        block = dn[q, 16 * i:16 * (i + 1)].reshape(512, 128).T
        for e in range(2):
            down_out[2 * q + e, :, 512 * i:512 * (i + 1)] = block[64 * e:64 * (e + 1), :]

    def wide(j):
        return pl.ds(0, 32 * DOWN[j][1])

    def core_copy(j):
        return remote(part.at[j, :, wide(j)], core_land.at[j, :, wide(j)], core_send.at[j], core_recv.at[j], (mate, t))

    def x_start(j):
        for d in (2, 1, 3):
            xd = lax.rem(x + d, NX)
            remote(xs.at[j, xd, :, wide(j)], x_land.at[j, d - 1, :, wide(j)], x_send.at[j], x_recv.at[j],
                   (z * (NX * NC) + xd * NC + c, t)).start()

    def x_all(j):
        return remote(xs.at[j, pl.ds(0, NX - 1), :, wide(j)], x_land.at[j, :, :, wide(j)], x_send.at[j], x_recv.at[j],
                      (mate, t))

    def z_start(j):
        for d in (4, 3, 5, 2, 6, 1, 7):
            zd = lax.rem(z + d, NZ)
            remote(zs.at[j, zd, :, wide(j)], z_land.at[j, d - 1, :, wide(j)], z_send.at[j], z_recv.at[j],
                   (zd * (NX * NC) + x * NC + c, t)).start()

    def z_all(j):
        return remote(zs.at[j, pl.ds(0, NZ - 1), :, wide(j)], z_land.at[j, :, :, wide(j)], z_send.at[j], z_recv.at[j],
                      (mate, t))

    def down_rows(j, side):
        first, count = DOWN[j]
        rows = pl.ds(pl.multiple_of(384 * side, 128), 384)
        block = jnp.concatenate([dn[q, first:first + count].reshape(32 * count, 128) for q in range(4)], axis=1)
        return lax.dot_general(hid[rows, :], block, (((1,), (1,)), ((), ())), preferred_element_type=F32)

    def forward(j):
        ag_forward(j + 3)
        if j + AHEAD < len(DOWN):
            ag_own(j + AHEAD + 3)

    def step_a(j):
        ag_arrived(j + 3, 2)
        ag_arrived(j + 3, 3)
        part[j, :, wide(j)] = down_rows(j, 1 - c).astype(BF16)
        core_copy(j).start()
        own[j % 2, :, wide(j)] = down_rows(j, c)

    def step_b(j):
        core_copy(j).wait_recv()
        for i in range(NX):
            rows = slice(96 * i, 96 * (i + 1))
            xs[j, i, :, wide(j)] = (
                own[j % 2, rows, wide(j)] + core_land[j, rows, wide(j)].astype(F32)).astype(BF16)
        x_start(j)

    def step_c(j):
        x_all(j).wait_recv()
        total = xs[j, x, :, wide(j)].astype(F32)
        for d in range(3):
            total += x_land[j, d, :, wide(j)].astype(F32)
        for zi in range(NZ):
            zs[j, zi, :, wide(j)] = total[12 * zi:12 * (zi + 1)].astype(BF16)
        z_start(j)

    def step_d(j):
        z_all(j).wait_recv()
        total = zs[j, z, :, wide(j)].astype(F32)
        for d in range(NZ - 1):
            total += z_land[j, d, :, wide(j)].astype(F32)
        first, count = DOWN[j]
        mixed[:, 32 * first:32 * (first + count)] = total.astype(BF16)

    scope = jax.named_scope
    with scope("begin"):
        small_copy(0).start()
        for i in range(3):
            raw_copy(i).start()
        barrier = enter()
        for i in (1, 2):
            small_copy(i).start()
        for i in range(NX):
            tok_copy(i).start()
        small_copy(0).wait()
    with scope("pack"):
        pack(0)
        pack(1)
    with scope("barrier"):
        pl.semaphore_wait(barrier, ALL + 2)
        for k in range(3):
            s1_start(k)
    with scope("pack_down"):
        pack(2)

    with scope("s1_0"):
        s1_wait(0)
        s1_start(3)
        s2_send_all(0)
    with scope("norm_0"):
        norm(0)
    with scope("s1_1"):
        s1_wait(1)
        s2_send_all(1)
    with scope("norm_1"):
        norm(1)
        norm(2)
    with scope("s1_2"):
        s1_wait(2)
        s2_send_all(2)
    with scope("norm_2"):
        norm(3)
    with scope("s2_0"):
        s2_all(0).wait_recv()
        ag_own(0)
    with scope("s1_3"):
        s1_wait(3)
        s2_send_all(3)
    with scope("gates"):
        spread_gates()
    with scope("s2_1"):
        s2_all(1).wait_recv()
        ag_own(1)
    with scope("fwd_0"):
        ag_forward(0)
    with scope("fwd_1"):
        ag_forward(1)
    with scope("s2_2"):
        s2_all(2).wait_recv()
        ag_own(2)
    with scope("hidden_t"):
        hidden(t)
    with scope("turn_t"):
        turn_both(t)
    with scope("fwd_2"):
        ag_forward(2)
    with scope("s2_3"):
        s2_all(3).wait_recv()
        for j in range(AHEAD):
            ag_own(3 + j)
    with scope("near"):
        for k in range(3):
            ag_arrived(k, 2)
    with scope("hidden_lr"):
        hidden(left)
        hidden(right)
    with scope("turn_lr"):
        turn_both(left)
        turn_both(right)
    with scope("far"):
        for k in range(3):
            ag_arrived(k, 3)
    with scope("hidden_far"):
        hidden(far)
    def turn_rest():
        turn_both(far)
        for q in range(4):
            for i in range(4):
                turn_down(q, i)

    steps = dict(F=forward, a=step_a, b=step_b, c=step_c, d=step_d)
    for step, j in order_of_steps():
        with scope(f"step_{step}{j}"):
            steps[step](j)
            if step == "b" and j == len(DOWN) - 1:
                turn_rest()

    with scope("drain"):
        for k in range(4):
            s1_all(k).wait_send()
            s2_all(k).wait_send()
        for k in range(3 + len(DOWN)):
            ag_sent(k)
        for j in range(len(DOWN)):
            core_copy(j).wait_send()
            x_all(j).wait_send()
            z_all(j).wait_send()


def exchange(gate, up, down, gain, tok, ids, mix):
    dma, vmem = pltpu.SemaphoreType.DMA, pltpu.VMEM
    whole = pl.BlockSpec(memory_space=pltpu.VMEM)
    serve = jax.ShapeDtypeStruct((8, 64, 2048), BF16)
    n, width = len(DOWN), 32 * max(count for _, count in DOWN)
    return pl.pallas_call(
        main_kernel,
        in_specs=[pl.BlockSpec(memory_space=pltpu.HBM)] * 7,
        out_specs=[whole] * 4,
        out_shape=(serve, serve, serve, jax.ShapeDtypeStruct((12, 2048), BF16)),
        scratch_shapes=[
            vmem((3, 8, 32, 1024), F32),
            vmem((1, 32), F32),
            vmem((2, 768), jnp.int32),
            vmem((2, 768), F32),
            vmem((4, 768, 128), F32),
            vmem((2, 4, 16, 16, 256), BF16),
            vmem((4, 16, 32, 128), BF16),
            vmem((2, 64, 16, 256), BF16),
            vmem((64, 32, 128), BF16),
            vmem((4, 64, 2, 16, 256), BF16),
            vmem((4, 64, 32, 128), BF16),
            vmem((NX, NZ, 24, 2048), BF16),
            vmem((768, 2048), BF16),
            vmem((768, 512), BF16),
            vmem((n, 384, width), BF16),
            vmem((2, 384, width), F32),
            vmem((n, 384, width), BF16),
            vmem((n, NX, 96, width), BF16),
            vmem((n, NX - 1, 96, width), BF16),
            vmem((n, NZ, 12, width), BF16),
            vmem((n, NZ - 1, 12, width), BF16),
            dma((4,)), dma((4,)),
            dma((4,)), dma((4,)),
            dma((3 + n,)), dma((3 + n, 4)),
            dma((n,)), dma((n,)),
            dma((n,)), dma((n,)),
            dma((n,)), dma((n,)),
            dma((10,)),
        ],
        compiler_params=pltpu.CompilerParams(
            has_side_effects=True, collective_id=0, vmem_limit_bytes=44 * 2**20),
    )(*(pltpu.with_memory_space_constraint(a, pltpu.HBM) for a in (gate, up, down, gain, tok, ids, mix)))


def copy_kernel(*refs):
    half = len(refs) // 2
    copies = [pltpu.make_async_copy(refs[i], refs[half + i], refs[-1].at[i]) for i in range(half)]
    for copy in copies:
        copy.start()
    for copy in copies:
        copy.wait()


def copied(arrays):
    anywhere = pl.BlockSpec(memory_space=pl.ANY)
    return pl.pallas_call(
        copy_kernel,
        in_specs=[anywhere] * len(arrays),
        out_specs=[pl.BlockSpec(memory_space=pltpu.HBM)] * len(arrays),
        out_shape=tuple(jax.ShapeDtypeStruct(a.shape, a.dtype) for a in arrays),
        scratch_shapes=[pltpu.SemaphoreType.DMA((len(arrays),))],
        compiler_params=pltpu.CompilerParams(vmem_limit_bytes=2**20),
    )(*arrays)


def local(tokens, norm_gain, gate_weight, up_weight, down_weight, expert_ids, expert_mix):
    *serve, mixed = copied(exchange(
        gate_weight, up_weight, down_weight, norm_gain[None, :], tokens.reshape(NZ, NX, 24, 2048),
        expert_ids.reshape(768, 2).T, expert_mix.reshape(768, 2).T))
    return tuple(jnp.swapaxes(out, 1, 2) for out in serve) + (mixed.reshape(12, 1, 2048),)


def solution(mesh):
    return jax.shard_map(
        local,
        mesh=mesh,
        in_specs=(
            P(None, "tp", None),
            P("fs"),
            P(None, "fs", "tp"),
            P(None, "fs", "tp"),
            P(None, "fs", "tp"),
            P(None, "tp", None),
            P(None, "tp", None),
        ),
        out_specs=(
            P(None, None, "fs"),
            P(None, None, "fs"),
            P(None, None, "fs"),
            P("fs", "tp", None),
        ),
        check_vma=False,
    )
```

```python
import functools

import jax
import jax.numpy as jnp
from jax import lax
from jax.experimental import pallas as pl
from jax.experimental.pallas import tpu as pltpu
from jax.sharding import PartitionSpec as P

norm_eps = 1e-05
MESH = pl.DeviceIdType.MESH
BF16, F32 = jnp.bfloat16, jnp.float32
NZ, NX, NC = 8, 4, 2


ALL = NZ * NX * NC
LANES = (slice(0, 128), slice(128, 256), slice(0, 256))
HALF = (0, 0, 1)
DOWN = tuple((8 * j, 8) for j in range(8))
AHEAD = 3


def order_of_steps():
    when, y, x, z = [], 0.0, 0.0, 0.0
    end = sum(count for _, count in DOWN) / 8 + 1.0
    for j, (_, count) in enumerate(DOWN):
        y += count / 8
        x = max(x, y + 0.9) + count / 8
        z = max(z, x + 1.5) + count / 16
        when += [(y - 2.8, 0, "F", j), (y, 1, "a", j), (y + 0.9, 2, "b", j), (x + 1.5, 3, "c", j),
                 (max(z + 2.2, end), 4, "d", j)]
    return [(step, j) for _, _, step, j in sorted(when)]


def main_kernel(gate_in, up_in, down_in, gain_in, tok, ids_in, mix_in, gate_out, up_out, down_out, mixed,
                raw, gainv, idsv, mixv, gates, pg, pd, lg, ld, wg, dn, tokv, normed, hid, part, own, core_land,
                xs, x_land, zs, z_land, s1_send, s1_recv, s2_send, s2_recv, ag_send, ag_recv,
                core_send, core_recv, x_send, x_recv, z_send, z_recv, in_sem):
    f, t = lax.axis_index("fs"), lax.axis_index("tp")
    z, x, c = lax.div(f, NX * NC), lax.rem(lax.div(f, NC), NX), lax.rem(f, NC)
    mate = f + 1 - 2 * c
    right, left, far = lax.rem(t + 1, 4), lax.rem(t + 3, 4), lax.rem(t + 2, 4)

    def remote(src, dst, send, recv, device):
        return pltpu.make_async_remote_copy(
            src_ref=src, dst_ref=dst, send_sem=send, recv_sem=recv, device_id=device, device_id_type=MESH)

    def others(act):
        def some(m, carry):
            for zi in range(NZ):
                zo = (zi + 1) // 2 if zi % 2 else NZ - zi // 2
                zd = lax.rem(z + zo, NZ)
                xd = lax.rem(x + lax.rem(m + zi, NX), NX)
                cd = lax.rem(c + lax.div(m, NX), NC)
                u = zd * (NX * NC) + xd * NC + cd
                if zi == 0:
                    pl.when(m > 0)(functools.partial(act, u))
                else:
                    act(u)
            return carry

        lax.fori_loop(0, NZ, some, 0)

    def enter():
        barrier = pltpu.get_barrier_semaphore()

        def greet(device):
            pl.semaphore_signal(barrier, inc=1, device_id=device, device_id_type=MESH)

        near = [lax.rem(x + xo, NX) * NC + lax.rem(c + co, NC) for xo in (2, 1, 3, 0) for co in range(NC)]
        for zo in (4, 3, 5, 2, 6, 1, 7, 0):
            base = lax.rem(z + zo, NZ) * (NX * NC)
            for n, u in enumerate(near):
                if zo or n != 2 * NX - 2:
                    greet((base + u, t))
        for d in (2, 1, 3):
            greet((f, lax.rem(t + d, 4)))
        return barrier

    def raw_copy(i):
        return pltpu.make_async_copy((gate_in, up_in, down_in)[i], raw.at[i], in_sem.at[i])

    def small_copy(i):
        src, dst = ((gain_in, gainv), (ids_in, idsv), (mix_in, mixv))[i]
        return pltpu.make_async_copy(src, dst, in_sem.at[3 + i])

    def tok_copy(i):
        return pltpu.make_async_copy(tok.at[:, i], tokv.at[i], in_sem.at[6 + i])

    def pack(i):
        low = lax.broadcasted_iota(jnp.int32, (32, 128), 1) < 64
        square = [lax.broadcasted_iota(jnp.int32, (32, 32), axis) for axis in (0, 1)]
        spread = jnp.where(square[0] == square[1], jnp.broadcast_to(gainv[...], (32, 32)), 0.0)
        scale = jnp.sum(spread, axis=1, keepdims=True)
        raw_copy(i).wait()

        def some(q, carry):
            for j in range(8):
                a, b = (raw[i, 2 * q + e, :, 128 * j:128 * (j + 1)] for e in range(2))
                if i < 2:
                    a, b = a * scale, b * scale
                even = jnp.where(low, a, pltpu.roll(b, 64, 1)).astype(BF16)
                odd = jnp.where(low, pltpu.roll(a, 64, 1), b).astype(BF16)
                for o, v in enumerate((even, odd)):
                    if i < 2:
                        for half in range(2):
                            pg[half, q, 2 * j + o, :, 128 * i:128 * (i + 1)] = v[16 * half:16 * (half + 1)]
                    else:
                        pd[q, 2 * j + o] = v
            return carry

        lax.fori_loop(0, 4, some, 0)
        if i < 2:
            for half in range(2):
                lanes = slice(128 * i, 128 * (i + 1))
                lg[half, pl.ds(16 * t, 16), :, lanes] = pg[half, t, :, :, lanes]
        else:
            ld[pl.ds(16 * t, 16)] = pd[t]

    def place(core):
        return lax.rem(core + c + 1, NC)

    def spread_gates():
        small_copy(1).wait()
        small_copy(2).wait()
        for q in range(4):
            sides = []
            for e in (2 * q, 2 * q + 1):
                row = sum(jnp.where(idsv[k:k + 1, :] == e, mixv[k:k + 1, :], 0.0) for k in range(2))
                sides.append(jnp.broadcast_to(row, (64, 768)))
            turned = jnp.concatenate(sides, axis=0).T
            for ci in range(NC):
                for xi in range(NX):
                    for zi in range(NZ):
                        at, by = 96 * xi + 12 * zi, 96 * zi + 24 * xi + 12 * ci
                        gates[q, place(ci), at:at + 12, :] = turned[by:by + 12, :]

    def s1(k, d):
        q = lax.rem(t + d, 4)
        sems = (s1_send.at[k // 3], s1_recv.at[k], (f, q))
        if k < 3:
            return remote(pg.at[HALF[k], q, :, :, LANES[k]], lg.at[HALF[k], pl.ds(16 * t, 16), :, LANES[k]], *sems)
        return remote(pd.at[q], ld.at[pl.ds(16 * t, 16)], *sems)

    def s1_start(k):
        for d in (2, 1, 3):
            s1(k, d).start()

    def s1_all(k):
        sems = (s1_send.at[k // 3], s1_recv.at[k], (f, right))
        if k < 3:
            return remote(pg.at[HALF[k], pl.ds(0, 3), :, :, LANES[k]], pg.at[HALF[k], pl.ds(0, 3), :, :, LANES[k]], *sems)
        return remote(pd.at[pl.ds(0, 3)], pd.at[pl.ds(0, 3)], *sems)

    def s1_wait(k):
        s1_all(k).wait_recv()

    def s2_send_all(k):
        def go(u):
            sems = (s2_send.at[k // 3], s2_recv.at[k], (u, t))
            if k < 3:
                remote(lg.at[HALF[k], u, :, LANES[k]], wg.at[t, f, HALF[k], :, LANES[k]], *sems).start()
            else:
                remote(ld.at[u], dn.at[t, f], *sems).start()

        others(go)
        if k < 3:
            wg[t, f, HALF[k], :, LANES[k]] = lg[HALF[k], f, :, LANES[k]]
        else:
            dn[t, f] = ld[f]

    def s2_all(k):
        blocks = pl.ds(0, ALL - 1)
        sems = (s2_send.at[k // 3], s2_recv.at[k], (mate, t))
        if k < 3:
            return remote(lg.at[HALF[k], blocks, :, LANES[k]], wg.at[t, blocks, HALF[k], :, LANES[k]], *sems)
        return remote(ld.at[blocks], dn.at[t, blocks], *sems)

    def ag_piece(k, q, piece):
        if k < 3:
            return wg.at[q, pl.ds(32 * piece, 32), HALF[k], :, LANES[k]]
        first, count = DOWN[k - 3]
        return dn.at[q, pl.ds(first + count // 2 * piece, count // 2)]

    def ag(k, slot):
        piece = (0, 1, 0, 1, 0, 1)[slot]
        to = (right, right, left, left, right, left)[slot]
        q = (t, t, t, t, left, right)[slot]
        ref = ag_piece(k, q, piece)
        return remote(ref, ref, ag_send.at[min(k, 3) // 3], ag_recv.at[k, (0, 2, 2, 1, 3, 3)[slot]], (f, to))

    def ag_own(k):
        for slot in (0, 3, 1, 2):
            ag(k, slot).start()

    def ag_arrived(k, group):
        if group < 2:
            ref = ag_piece(k, (left, right)[group], group)
        elif k < 3:
            ref = wg.at[far, :, HALF[k], :, LANES[k]]
        else:
            ref = dn.at[far, pl.ds(*DOWN[k - 3])]
        remote(ref, ref, ag_send.at[min(k, 3) // 3], ag_recv.at[k, group], (f, right)).wait_recv()

    def ag_forward(k):
        ag_arrived(k, 0)
        ag(k, 4).start()
        ag_arrived(k, 1)
        ag(k, 5).start()

    def norm(i):
        tok_copy(i).wait()

        def four(a, carry):
            v = jnp.concatenate([tokv[i, 4 * a + b].astype(F32) for b in range(4)], axis=0)
            mean = jnp.mean(v, axis=1, keepdims=True)
            v = v - mean
            var = jnp.mean(v * v, axis=1, keepdims=True)
            v = v * lax.rsqrt(var + norm_eps)
            for ci in range(NC):
                some = jnp.concatenate([v[24 * b + 12 * ci:24 * b + 12 * (ci + 1)] for b in range(4)], axis=0)
                rows = pl.ds(pl.multiple_of(96 * i + 48 * a, 16), 48)
                normed[place(ci), rows, :] = some.astype(BF16)
            return carry

        lax.fori_loop(0, NZ // 4, four, 0)

    def hidden(q):
        def some(r, carry):
            act = jnp.dot(normed[r], wg[q].reshape(2048, 256), preferred_element_type=F32)
            gate_act, up_act = act[:, :128], act[:, 128:]
            value = gate_act / (1.0 + jnp.exp(-gate_act)) * up_act * gates[q, r]
            hid[r, :, pl.ds(pl.multiple_of(q * 128, 128), 128)] = value.astype(BF16)
            return carry

        lax.fori_loop(0, NC, some, 0)

    def turn_both(q):
        for i in range(4):
            both = wg[q, 16 * i:16 * (i + 1)].reshape(512, 256).T
            for n, out in enumerate((gate_out, up_out)):
                for e in range(2):
                    out[2 * q + e, :, 512 * i:512 * (i + 1)] = both[128 * n + 64 * e:128 * n + 64 * (e + 1), :]

    def wide(j):
        return pl.ds(0, 32 * DOWN[j][1])

    def core_copy(j):
        return remote(part.at[j, :, wide(j)], core_land.at[j, :, wide(j)], core_send.at[0], core_recv.at[j], (mate, t))

    def x_start(j):
        for d in (2, 1, 3):
            xd = lax.rem(x + d, NX)
            remote(xs.at[j, xd, :, wide(j)], x_land.at[j, d - 1, :, wide(j)], x_send.at[0], x_recv.at[j],
                   (z * (NX * NC) + xd * NC + c, t)).start()

    def x_all(j):
        return remote(xs.at[j, pl.ds(0, NX - 1), :, wide(j)], x_land.at[j, :, :, wide(j)], x_send.at[0], x_recv.at[j],
                      (mate, t))

    def z_start(j):
        for d in (4, 3, 5, 2, 6, 1, 7):
            zd = lax.rem(z + d, NZ)
            remote(zs.at[j, zd, :, wide(j)], z_land.at[j, d - 1, :, wide(j)], z_send.at[0], z_recv.at[j],
                   (zd * (NX * NC) + x * NC + c, t)).start()

    def z_all(j):
        return remote(zs.at[j, pl.ds(0, NZ - 1), :, wide(j)], z_land.at[j, :, :, wide(j)], z_send.at[0], z_recv.at[j],
                      (mate, t))

    def forward(j):
        ag_forward(j + 3)
        if j + AHEAD < len(DOWN):
            ag_own(j + AHEAD + 3)

    def step_a(j):
        ag_arrived(j + 3, 2)
        ag_arrived(j + 3, 3)
        first, count = DOWN[j]
        turned = [dn[q, first:first + count].reshape(32 * count, 128).T for q in range(4)]
        block = jnp.concatenate(turned, axis=0)
        total = jnp.dot(hid[...].reshape(768, 512), block, preferred_element_type=F32)
        part[j, :, wide(j)] = total[:384].astype(BF16)
        core_copy(j).start()
        own[j % 2, :, wide(j)] = total[384:]
        for q in range(4):
            for e in range(2):
                down_out[2 * q + e, :, 32 * first:32 * (first + count)] = turned[q][64 * e:64 * (e + 1), :]

    def step_b(j):
        core_copy(j).wait_recv()
        for i in range(NX):
            rows = slice(96 * i, 96 * (i + 1))
            xs[j, i, :, wide(j)] = (
                own[j % 2, rows, wide(j)] + core_land[j, rows, wide(j)].astype(F32)).astype(BF16)
        x_start(j)

    def step_c(j):
        x_all(j).wait_recv()
        total = xs[j, x, :, wide(j)].astype(F32)
        for d in range(3):
            total += x_land[j, d, :, wide(j)].astype(F32)
        for zi in range(NZ):
            zs[j, zi, :, wide(j)] = total[12 * zi:12 * (zi + 1)].astype(BF16)
        z_start(j)

    def step_d(j):
        z_all(j).wait_recv()
        total = zs[j, z, :, wide(j)].astype(F32)
        for d in range(NZ - 1):
            total += z_land[j, d, :, wide(j)].astype(F32)
        first, count = DOWN[j]
        mixed[:, 32 * first:32 * (first + count)] = total.astype(BF16)

    scope = jax.named_scope
    with scope("begin"):
        small_copy(0).start()
        raw_copy(0).start()
        barrier = enter()
        for i in (1, 2):
            raw_copy(i).start()
            small_copy(i).start()
        for i in range(NX):
            tok_copy(i).start()
        small_copy(0).wait()
    with scope("pack"):
        pack(0)
    with scope("barrier"):
        pl.semaphore_wait(barrier, ALL + 2)
        s1_start(0)
    with scope("pack_rest"):
        pack(1)
        pack(2)
        s1_start(1)
        s1_start(2)

    with scope("s1_0"):
        s1_wait(0)
        s1_start(3)
        s2_send_all(0)
    with scope("norm_0"):
        norm(0)
    with scope("s1_1"):
        s1_wait(1)
        s2_send_all(1)
    with scope("norm_1"):
        norm(1)
        norm(2)
    with scope("s1_2"):
        s1_wait(2)
        s2_send_all(2)
    with scope("norm_2"):
        norm(3)
    with scope("s2_0"):
        s2_all(0).wait_recv()
        ag_own(0)
    with scope("s1_3"):
        s1_wait(3)
        s2_send_all(3)
    with scope("gates"):
        spread_gates()
    with scope("s2_1"):
        s2_all(1).wait_recv()
        ag_own(1)
    with scope("fwd_0"):
        ag_forward(0)
    with scope("fwd_1"):
        ag_forward(1)
    with scope("s2_2"):
        s2_all(2).wait_recv()
        ag_own(2)
    with scope("hidden_t"):
        hidden(t)
    with scope("turn_t"):
        turn_both(t)
    with scope("fwd_2"):
        ag_forward(2)
    with scope("s2_3"):
        s2_all(3).wait_recv()
        for j in range(AHEAD):
            ag_own(3 + j)
    with scope("near"):
        for k in range(3):
            ag_arrived(k, 2)
    with scope("hidden_lr"):
        hidden(left)
        hidden(right)
    with scope("turn_lr"):
        turn_both(left)
        turn_both(right)
    with scope("far"):
        for k in range(3):
            ag_arrived(k, 3)
    with scope("hidden_far"):
        hidden(far)
    steps = dict(F=forward, a=step_a, b=step_b, c=step_c, d=step_d)
    for step, j in order_of_steps():
        with scope(f"step_{step}{j}"):
            steps[step](j)
            if step == "b" and j == len(DOWN) - 1:
                turn_both(far)

    with scope("drain"):
        def sent(ref, sem):
            remote(ref, ref, sem, s1_recv.at[0], (mate, t)).wait_send()

        sent(pg.at[:, pl.ds(0, 3)], s1_send.at[0])
        sent(pd.at[pl.ds(0, 3)], s1_send.at[1])
        sent(wg.at[0, pl.ds(0, ALL - 1)], s2_send.at[0])
        sent(dn.at[0, pl.ds(0, ALL - 1)], s2_send.at[1])
        sent(wg.at[pl.ds(0, 3)], ag_send.at[0])
        sent(dn.at[pl.ds(0, 3)], ag_send.at[1])
        if len({count for _, count in DOWN}) > 1:
            for j in range(len(DOWN)):
                sent(part.at[j, :, wide(j)], core_send.at[0])
                sent(x_land.at[j, :, :, wide(j)], x_send.at[0])
                sent(z_land.at[j, :, :, wide(j)], z_send.at[0])
        else:
            sent(part, core_send.at[0])
            sent(x_land, x_send.at[0])
            sent(z_land, z_send.at[0])


def exchange(gate, up, down, gain, tok, ids, mix):
    dma, vmem = pltpu.SemaphoreType.DMA, pltpu.VMEM
    whole = pl.BlockSpec(memory_space=pltpu.VMEM)
    serve = jax.ShapeDtypeStruct((8, 64, 2048), BF16)
    n, width = len(DOWN), 32 * max(count for _, count in DOWN)
    return pl.pallas_call(
        main_kernel,
        in_specs=[pl.BlockSpec(memory_space=pltpu.HBM)] * 7,
        out_specs=[whole] * 4,
        out_shape=(serve, serve, serve, jax.ShapeDtypeStruct((12, 2048), BF16)),
        scratch_shapes=[
            vmem((3, 8, 32, 1024), F32),
            vmem((1, 32), F32),
            vmem((2, 768), jnp.int32),
            vmem((2, 768), F32),
            vmem((4, NC, 384, 128), F32),
            vmem((2, 4, 16, 16, 256), BF16),
            vmem((4, 16, 32, 128), BF16),
            vmem((2, 64, 16, 256), BF16),
            vmem((64, 32, 128), BF16),
            vmem((4, 64, 2, 16, 256), BF16),
            vmem((4, 64, 32, 128), BF16),
            vmem((NX, NZ, 24, 2048), BF16),
            vmem((NC, 384, 2048), BF16),
            vmem((NC, 384, 512), BF16),
            vmem((n, 384, width), BF16),
            vmem((2, 384, width), F32),
            vmem((n, 384, width), BF16),
            vmem((n, NX, 96, width), BF16),
            vmem((n, NX - 1, 96, width), BF16),
            vmem((n, NZ, 12, width), BF16),
            vmem((n, NZ - 1, 12, width), BF16),
            dma((2,)), dma((4,)),
            dma((2,)), dma((4,)),
            dma((2,)), dma((3 + n, 4)),
            dma((1,)), dma((n,)),
            dma((1,)), dma((n,)),
            dma((1,)), dma((n,)),
            dma((10,)),
        ],
        compiler_params=pltpu.CompilerParams(
            has_side_effects=True, collective_id=0, vmem_limit_bytes=44 * 2**20),
    )(*(pltpu.with_memory_space_constraint(a, pltpu.HBM) for a in (gate, up, down, gain, tok, ids, mix)))


def copy_kernel(*refs):
    half = len(refs) // 2
    copies = []
    for src, dst in zip(refs[:half], refs[half:]):
        pieces = [slice(None)] if src.ndim == 2 else [pl.ds(i, 2) for i in range(0, src.shape[0], 2)]
        copies += [pltpu.make_async_copy(src.at[p], dst.at[p], refs[-1].at[len(copies) + n]) for n, p in enumerate(pieces)]
    for copy in copies:
        copy.start()
    for copy in copies:
        copy.wait()


def copied(arrays):
    anywhere = pl.BlockSpec(memory_space=pl.ANY)
    return pl.pallas_call(
        copy_kernel,
        in_specs=[anywhere] * len(arrays),
        out_specs=[pl.BlockSpec(memory_space=pltpu.HBM)] * len(arrays),
        out_shape=tuple(jax.ShapeDtypeStruct(a.shape, a.dtype) for a in arrays),
        scratch_shapes=[pltpu.SemaphoreType.DMA((13,))],
        compiler_params=pltpu.CompilerParams(vmem_limit_bytes=2**20),
    )(*arrays)


def local(tokens, norm_gain, gate_weight, up_weight, down_weight, expert_ids, expert_mix):
    *serve, mixed = copied(exchange(
        gate_weight, up_weight, down_weight, norm_gain[None, :], tokens.reshape(NZ, NX, 24, 2048),
        expert_ids.reshape(768, 2).T, expert_mix.reshape(768, 2).T))
    return tuple(jnp.swapaxes(out, 1, 2) for out in serve) + (mixed.reshape(12, 1, 2048),)


def solution(mesh):
    return jax.shard_map(
        local,
        mesh=mesh,
        in_specs=(
            P(None, "tp", None),
            P("fs"),
            P(None, "fs", "tp"),
            P(None, "fs", "tp"),
            P(None, "fs", "tp"),
            P(None, "tp", None),
            P(None, "tp", None),
        ),
        out_specs=(
            P(None, None, "fs"),
            P(None, None, "fs"),
            P(None, None, "fs"),
            P("fs", "tp", None),
        ),
        check_vma=False,
    )
```

```python
import functools

import jax
import jax.numpy as jnp
from jax import lax
from jax.experimental import pallas as pl
from jax.experimental.pallas import tpu as pltpu
from jax.sharding import PartitionSpec as P

norm_eps = 1e-05
MESH = pl.DeviceIdType.MESH
BF16, F32 = jnp.bfloat16, jnp.float32
NZ, NX, NC = 8, 4, 2


ALL = NZ * NX * NC
LANES = (slice(0, 128), slice(128, 256), slice(0, 256))
HALF = (0, 0, 1)
DOWN = tuple((8 * j, 8) for j in range(8))
AHEAD = 2


def order_of_steps():
    sizes = [count / 8 for _, count in DOWN]
    own, when, y, x = [-1.0] * AHEAD, [], 0.0, 0.0
    for j, size in enumerate(sizes):
        if j >= AHEAD:
            when.append((own[j] + 0.8, 0, "F", j))
        y = max(y, own[j] + 0.8) + size / 3
        done = y + 0.8
        if j + AHEAD < len(DOWN):
            y += 2 * sizes[j + AHEAD] / 3
            own.append(y)
        x = max(x, done + 0.8) + size
        when += [(done, 1, "a", j), (done + 0.8, 2, "b", j), (x + 1.5, 3, "c", j), (x + 100, 4, "d", j)]
    return [(step, j) for _, _, step, j in sorted(when)]


def main_kernel(gate_in, up_in, down_in, gain_in, tok, ids_in, mix_in, gate_out, up_out, down_out, mixed,
                raw, gainv, idsv, mixv, gates, pg, pd, lg, ld, wg, dn, tokv, normed, hid, part, own, core_land,
                xs, x_land, zs, z_land, s1_send, s1_recv, s2_send, s2_recv, ag_send, ag_recv,
                core_send, core_recv, x_send, x_recv, z_send, z_recv, in_sem):
    f, t = lax.axis_index("fs"), lax.axis_index("tp")
    z, x, c = lax.div(f, NX * NC), lax.rem(lax.div(f, NC), NX), lax.rem(f, NC)
    mate = f + 1 - 2 * c
    right, left, far = lax.rem(t + 1, 4), lax.rem(t + 3, 4), lax.rem(t + 2, 4)

    def remote(src, dst, send, recv, device):
        return pltpu.make_async_remote_copy(
            src_ref=src, dst_ref=dst, send_sem=send, recv_sem=recv, device_id=device, device_id_type=MESH)

    def others(act):
        def some(m, carry):
            for zi in range(NZ):
                zo = (zi + 1) // 2 if zi % 2 else NZ - zi // 2
                zd = lax.rem(z + zo, NZ)
                xd = lax.rem(x + lax.rem(m + zi, NX), NX)
                cd = lax.rem(c + lax.div(m, NX), NC)
                u = zd * (NX * NC) + xd * NC + cd
                if zi == 0:
                    pl.when(m > 0)(functools.partial(act, u))
                else:
                    act(u)
            return carry

        lax.fori_loop(0, NZ, some, 0)

    def enter():
        barrier = pltpu.get_barrier_semaphore()

        def greet(device):
            pl.semaphore_signal(barrier, inc=1, device_id=device, device_id_type=MESH)

        near = [lax.rem(x + xo, NX) * NC + lax.rem(c + co, NC) for xo in (2, 1, 3, 0) for co in range(NC)]
        for zo in (4, 3, 5, 2, 6, 1, 7, 0):
            base = lax.rem(z + zo, NZ) * (NX * NC)
            for n, u in enumerate(near):
                if zo or n != 2 * NX - 2:
                    greet((base + u, t))
        for d in (2, 1, 3):
            greet((f, lax.rem(t + d, 4)))
        return barrier

    def raw_copy(i):
        return pltpu.make_async_copy((gate_in, up_in, down_in)[i], raw.at[i], in_sem.at[i])

    def small_copy(i):
        src, dst = ((gain_in, gainv), (ids_in, idsv), (mix_in, mixv))[i]
        return pltpu.make_async_copy(src, dst, in_sem.at[3 + i])

    def tok_copy(i):
        return pltpu.make_async_copy(tok.at[:, i], tokv.at[i], in_sem.at[6 + i])

    def pack(i):
        low = lax.broadcasted_iota(jnp.int32, (32, 128), 1) < 64
        square = [lax.broadcasted_iota(jnp.int32, (32, 32), axis) for axis in (0, 1)]
        spread = jnp.where(square[0] == square[1], jnp.broadcast_to(gainv[...], (32, 32)), 0.0)
        scale = jnp.sum(spread, axis=1, keepdims=True)
        raw_copy(i).wait()

        def some(q, carry):
            for j in range(8):
                a, b = (raw[i, 2 * q + e, :, 128 * j:128 * (j + 1)] for e in range(2))
                if i < 2:
                    a, b = a * scale, b * scale
                even = jnp.where(low, a, pltpu.roll(b, 64, 1)).astype(BF16)
                odd = jnp.where(low, pltpu.roll(a, 64, 1), b).astype(BF16)
                for o, v in enumerate((even, odd)):
                    if i < 2:
                        for half in range(2):
                            pg[half, q, 2 * j + o, :, 128 * i:128 * (i + 1)] = v[16 * half:16 * (half + 1)]
                    else:
                        pd[q, 2 * j + o] = v
            return carry

        lax.fori_loop(0, 4, some, 0)
        if i < 2:
            for half in range(2):
                lanes = slice(128 * i, 128 * (i + 1))
                lg[half, pl.ds(16 * t, 16), :, lanes] = pg[half, t, :, :, lanes]
        else:
            ld[pl.ds(16 * t, 16)] = pd[t]

    def place(core):
        return lax.rem(core + c + 1, NC)

    def spread_gates():
        small_copy(1).wait()
        small_copy(2).wait()
        for q in range(4):
            sides = []
            for e in (2 * q, 2 * q + 1):
                row = sum(jnp.where(idsv[k:k + 1, :] == e, mixv[k:k + 1, :], 0.0) for k in range(2))
                sides.append(jnp.broadcast_to(row, (64, 768)))
            turned = jnp.concatenate(sides, axis=0).T
            for ci in range(NC):
                for xi in range(NX):
                    for zi in range(NZ):
                        at, by = 96 * xi + 12 * zi, 96 * zi + 24 * xi + 12 * ci
                        gates[q, place(ci), at:at + 12, :] = turned[by:by + 12, :]

    def s1(k, d):
        q = lax.rem(t + d, 4)
        sems = (s1_send.at[k // 3], s1_recv.at[k], (f, q))
        if k < 3:
            return remote(pg.at[HALF[k], q, :, :, LANES[k]], lg.at[HALF[k], pl.ds(16 * t, 16), :, LANES[k]], *sems)
        return remote(pd.at[q], ld.at[pl.ds(16 * t, 16)], *sems)

    def s1_start(k):
        for d in (2, 1, 3):
            s1(k, d).start()

    def s1_all(k):
        sems = (s1_send.at[k // 3], s1_recv.at[k], (f, right))
        if k < 3:
            return remote(pg.at[HALF[k], pl.ds(0, 3), :, :, LANES[k]], pg.at[HALF[k], pl.ds(0, 3), :, :, LANES[k]], *sems)
        return remote(pd.at[pl.ds(0, 3)], pd.at[pl.ds(0, 3)], *sems)

    def s1_wait(k):
        s1_all(k).wait_recv()

    def s2_send_all(k):
        def go(u):
            sems = (s2_send.at[k // 3], s2_recv.at[k], (u, t))
            if k < 3:
                remote(lg.at[HALF[k], u, :, LANES[k]], wg.at[t, f, HALF[k], :, LANES[k]], *sems).start()
            else:
                remote(ld.at[u], dn.at[t, f], *sems).start()

        others(go)
        if k < 3:
            wg[t, f, HALF[k], :, LANES[k]] = lg[HALF[k], f, :, LANES[k]]
        else:
            dn[t, f] = ld[f]

    def s2_all(k):
        blocks = pl.ds(0, ALL - 1)
        sems = (s2_send.at[k // 3], s2_recv.at[k], (mate, t))
        if k < 3:
            return remote(lg.at[HALF[k], blocks, :, LANES[k]], wg.at[t, blocks, HALF[k], :, LANES[k]], *sems)
        return remote(ld.at[blocks], dn.at[t, blocks], *sems)

    def ag_piece(k, q, piece):
        if k < 3:
            return wg.at[q, pl.ds(32 * piece, 32), HALF[k], :, LANES[k]]
        first, count = DOWN[k - 3]
        return dn.at[q, pl.ds(first + count // 2 * piece, count // 2)]

    def ag_group(k, group):
        return 4 * k + group if k < 3 else 12 + 3 * (k - 3) + min(group, 2)

    def ag(k, slot):
        piece = (0, 1, 0, 1, 0, 1)[slot]
        to = (right, right, left, left, right, left)[slot]
        q = (t, t, t, t, left, right)[slot]
        ref = ag_piece(k, q, piece)
        return remote(ref, ref, ag_send.at[min(k, 3) // 3], ag_recv.at[ag_group(k, (0, 2, 2, 1, 3, 3)[slot])], (f, to))

    def ag_own(k):
        for slot in (0, 3, 1, 2):
            ag(k, slot).start()

    def ag_arrived(k, group):
        if group < 2:
            ref = ag_piece(k, (left, right)[group], group)
        elif k < 3:
            ref = wg.at[far, :, HALF[k], :, LANES[k]]
        else:
            ref = dn.at[pl.ds(0, 2), pl.ds(*DOWN[k - 3])]
        remote(ref, ref, ag_send.at[min(k, 3) // 3], ag_recv.at[ag_group(k, group)], (f, right)).wait_recv()

    def ag_forward(k):
        ag_arrived(k, 0)
        ag(k, 4).start()
        ag_arrived(k, 1)
        ag(k, 5).start()

    def norm(i):
        tok_copy(i).wait()

        def four(a, carry):
            v = jnp.concatenate([tokv[i, 4 * a + b].astype(F32) for b in range(4)], axis=0)
            mean = jnp.mean(v, axis=1, keepdims=True)
            v = v - mean
            var = jnp.mean(v * v, axis=1, keepdims=True)
            v = v * lax.rsqrt(var + norm_eps)
            for ci in range(NC):
                some = jnp.concatenate([v[24 * b + 12 * ci:24 * b + 12 * (ci + 1)] for b in range(4)], axis=0)
                rows = pl.ds(pl.multiple_of(96 * i + 48 * a, 16), 48)
                normed[place(ci), rows, :] = some.astype(BF16)
            return carry

        lax.fori_loop(0, NZ // 4, four, 0)

    def hidden(q):
        def some(r, carry):
            act = jnp.dot(normed[r], wg[q].reshape(2048, 256), preferred_element_type=F32)
            gate_act, up_act = act[:, :128], act[:, 128:]
            value = gate_act / (1.0 + jnp.exp(-gate_act)) * up_act * gates[q, r]
            hid[r, :, pl.ds(pl.multiple_of(q * 128, 128), 128)] = value.astype(BF16)
            return carry

        lax.fori_loop(0, NC, some, 0)

    def turn_both(q):
        for i in range(4):
            both = wg[q, 16 * i:16 * (i + 1)].reshape(512, 256).T
            for n, out in enumerate((gate_out, up_out)):
                for e in range(2):
                    out[2 * q + e, :, 512 * i:512 * (i + 1)] = both[128 * n + 64 * e:128 * n + 64 * (e + 1), :]

    def wide(j):
        return pl.ds(0, 32 * DOWN[j][1])

    def core_copy(j):
        return remote(part.at[j, :, wide(j)], core_land.at[j, :, wide(j)], core_send.at[0], core_recv.at[j], (mate, t))

    def x_start(j):
        for d in (2, 1, 3):
            xd = lax.rem(x + d, NX)
            remote(xs.at[j, xd, :, wide(j)], x_land.at[j, d - 1, :, wide(j)], x_send.at[0], x_recv.at[j],
                   (z * (NX * NC) + xd * NC + c, t)).start()

    def x_all(j):
        return remote(xs.at[j, pl.ds(0, NX - 1), :, wide(j)], x_land.at[j, :, :, wide(j)], x_send.at[0], x_recv.at[j],
                      (mate, t))

    def z_start(j):
        for d in (4, 3, 5, 2, 6, 1, 7):
            zd = lax.rem(z + d, NZ)
            remote(zs.at[j, zd, :, wide(j)], z_land.at[j, d - 1, :, wide(j)], z_send.at[0], z_recv.at[j],
                   (zd * (NX * NC) + x * NC + c, t)).start()

    def z_all(j):
        return remote(zs.at[j, pl.ds(0, NZ - 1), :, wide(j)], z_land.at[j, :, :, wide(j)], z_send.at[0], z_recv.at[j],
                      (mate, t))

    def forward(j):
        ag_forward(j + 3)
        if j + AHEAD < len(DOWN):
            ag_own(j + AHEAD + 3)

    def step_a(j):
        ag_arrived(j + 3, 2)
        first, count = DOWN[j]
        turned = [dn[q, first:first + count].reshape(32 * count, 128).T for q in range(4)]
        block = jnp.concatenate(turned, axis=0)
        total = jnp.dot(hid[...].reshape(768, 512), block, preferred_element_type=F32)
        part[j, :, wide(j)] = total[:384].astype(BF16)
        core_copy(j).start()
        own[j % 2, :, wide(j)] = total[384:]
        for q in range(4):
            for e in range(2):
                down_out[2 * q + e, :, 32 * first:32 * (first + count)] = turned[q][64 * e:64 * (e + 1), :]

    def step_b(j):
        core_copy(j).wait_recv()
        for i in range(NX):
            rows = slice(96 * i, 96 * (i + 1))
            xs[j, i, :, wide(j)] = (
                own[j % 2, rows, wide(j)] + core_land[j, rows, wide(j)].astype(F32)).astype(BF16)
        x_start(j)

    def step_c(j):
        x_all(j).wait_recv()
        total = xs[j, x, :, wide(j)].astype(F32)
        for d in range(3):
            total += x_land[j, d, :, wide(j)].astype(F32)
        for zi in range(NZ):
            zs[j, zi, :, wide(j)] = total[12 * zi:12 * (zi + 1)].astype(BF16)
        z_start(j)

    def step_d(j):
        z_all(j).wait_recv()
        total = zs[j, z, :, wide(j)].astype(F32)
        for d in range(NZ - 1):
            total += z_land[j, d, :, wide(j)].astype(F32)
        first, count = DOWN[j]
        mixed[:, 32 * first:32 * (first + count)] = total.astype(BF16)

    scope = jax.named_scope
    with scope("begin"):
        small_copy(0).start()
        raw_copy(0).start()
        barrier = enter()
        for i in (1, 2):
            raw_copy(i).start()
            small_copy(i).start()
        for i in range(NX):
            tok_copy(i).start()
        small_copy(0).wait()
    with scope("pack"):
        pack(0)
    with scope("barrier"):
        pl.semaphore_wait(barrier, ALL + 2)
        s1_start(0)
    with scope("pack_rest"):
        pack(1)
        pack(2)
        s1_start(1)
        s1_start(2)

    with scope("s1_0"):
        s1_wait(0)
        s1_start(3)
        s2_send_all(0)
    with scope("norm_0"):
        norm(0)
    with scope("s1_1"):
        s1_wait(1)
        s2_send_all(1)
    with scope("norm_1"):
        norm(1)
        norm(2)
    with scope("s1_2"):
        s1_wait(2)
        s2_send_all(2)
    with scope("norm_2"):
        norm(3)
    with scope("s2_0"):
        s2_all(0).wait_recv()
        ag_own(0)
    with scope("s1_3"):
        s1_wait(3)
        s2_send_all(3)
    with scope("gates"):
        spread_gates()
    with scope("s2_1"):
        s2_all(1).wait_recv()
        ag_own(1)
    with scope("fwd_0"):
        ag_forward(0)
    with scope("fwd_1"):
        ag_forward(1)
    with scope("s2_2"):
        s2_all(2).wait_recv()
        ag_own(2)
    with scope("hidden_t"):
        hidden(t)
    with scope("turn_t"):
        turn_both(t)
    with scope("s2_3"):
        s2_all(3).wait_recv()
        for j in range(AHEAD):
            ag_own(3 + j)
    with scope("fwd_2"):
        ag_forward(2)
    with scope("near"):
        for k in range(3):
            ag_arrived(k, 2)
    with scope("hidden_lr"):
        hidden(left)
        hidden(right)
    with scope("turn_lr"):
        turn_both(left)
        turn_both(right)
    with scope("fwd_down"):
        for j in range(AHEAD):
            forward(j)
    with scope("far"):
        for k in range(3):
            ag_arrived(k, 3)
    with scope("hidden_far"):
        hidden(far)
    steps = dict(F=forward, a=step_a, b=step_b, c=step_c, d=step_d)
    for step, j in order_of_steps():
        with scope(f"step_{step}{j}"):
            steps[step](j)
            if step == "b" and j == len(DOWN) - 1:
                turn_both(far)

    with scope("drain"):
        def sent(ref, sem):
            remote(ref, ref, sem, s1_recv.at[0], (mate, t)).wait_send()

        sent(pg.at[:, pl.ds(0, 3)], s1_send.at[0])
        sent(pd.at[pl.ds(0, 3)], s1_send.at[1])
        sent(wg.at[0, pl.ds(0, ALL - 1)], s2_send.at[0])
        sent(dn.at[0, pl.ds(0, ALL - 1)], s2_send.at[1])
        sent(wg.at[pl.ds(0, 3)], ag_send.at[0])
        sent(dn.at[pl.ds(0, 3)], ag_send.at[1])
        if len({count for _, count in DOWN}) > 1:
            for j in range(len(DOWN)):
                sent(part.at[j, :, wide(j)], core_send.at[0])
                sent(x_land.at[j, :, :, wide(j)], x_send.at[0])
                sent(z_land.at[j, :, :, wide(j)], z_send.at[0])
        else:
            sent(part, core_send.at[0])
            sent(x_land, x_send.at[0])
            sent(z_land, z_send.at[0])


def exchange(gate, up, down, gain, tok, ids, mix):
    dma, vmem = pltpu.SemaphoreType.DMA, pltpu.VMEM
    whole = pl.BlockSpec(memory_space=pltpu.VMEM)
    serve = jax.ShapeDtypeStruct((8, 64, 2048), BF16)
    n, width = len(DOWN), 32 * max(count for _, count in DOWN)
    return pl.pallas_call(
        main_kernel,
        in_specs=[pl.BlockSpec(memory_space=pltpu.HBM)] * 7,
        out_specs=[whole] * 4,
        out_shape=(serve, serve, serve, jax.ShapeDtypeStruct((12, 2048), BF16)),
        scratch_shapes=[
            vmem((3, 8, 32, 1024), F32),
            vmem((1, 32), F32),
            vmem((2, 768), jnp.int32),
            vmem((2, 768), F32),
            vmem((4, NC, 384, 128), F32),
            vmem((2, 4, 16, 16, 256), BF16),
            vmem((4, 16, 32, 128), BF16),
            vmem((2, 64, 16, 256), BF16),
            vmem((64, 32, 128), BF16),
            vmem((4, 64, 2, 16, 256), BF16),
            vmem((4, 64, 32, 128), BF16),
            vmem((NX, NZ, 24, 2048), BF16),
            vmem((NC, 384, 2048), BF16),
            vmem((NC, 384, 512), BF16),
            vmem((n, 384, width), BF16),
            vmem((2, 384, width), F32),
            vmem((n, 384, width), BF16),
            vmem((n, NX, 96, width), BF16),
            vmem((n, NX - 1, 96, width), BF16),
            vmem((n, NZ, 12, width), BF16),
            vmem((n, NZ - 1, 12, width), BF16),
            dma((2,)), dma((4,)),
            dma((2,)), dma((4,)),
            dma((2,)), dma((12 + 3 * n,)),
            dma((1,)), dma((n,)),
            dma((1,)), dma((n,)),
            dma((1,)), dma((n,)),
            dma((10,)),
        ],
        compiler_params=pltpu.CompilerParams(
            has_side_effects=True, collective_id=0, vmem_limit_bytes=44 * 2**20),
    )(*(pltpu.with_memory_space_constraint(a, pltpu.HBM) for a in (gate, up, down, gain, tok, ids, mix)))


def copy_kernel(*refs):
    half = len(refs) // 2
    copies = []
    for src, dst in zip(refs[:half], refs[half:]):
        pieces = [slice(None)] if src.ndim == 2 else [pl.ds(i, 4) for i in range(0, src.shape[0], 4)]
        copies += [pltpu.make_async_copy(src.at[p], dst.at[p], refs[-1].at[len(copies) + n]) for n, p in enumerate(pieces)]
    for copy in copies:
        copy.start()
    for copy in copies:
        copy.wait()


def copied(arrays):
    anywhere = pl.BlockSpec(memory_space=pl.ANY)
    return pl.pallas_call(
        copy_kernel,
        in_specs=[anywhere] * len(arrays),
        out_specs=[pl.BlockSpec(memory_space=pltpu.HBM)] * len(arrays),
        out_shape=tuple(jax.ShapeDtypeStruct(a.shape, a.dtype) for a in arrays),
        scratch_shapes=[pltpu.SemaphoreType.DMA((7,))],
        compiler_params=pltpu.CompilerParams(vmem_limit_bytes=2**20),
    )(*arrays)


def local(tokens, norm_gain, gate_weight, up_weight, down_weight, expert_ids, expert_mix):
    *serve, mixed = copied(exchange(
        gate_weight, up_weight, down_weight, norm_gain[None, :], tokens.reshape(NZ, NX, 24, 2048),
        expert_ids.reshape(768, 2).T, expert_mix.reshape(768, 2).T))
    return tuple(jnp.swapaxes(out, 1, 2) for out in serve) + (mixed.reshape(12, 1, 2048),)


def solution(mesh):
    return jax.shard_map(
        local,
        mesh=mesh,
        in_specs=(
            P(None, "tp", None),
            P("fs"),
            P(None, "fs", "tp"),
            P(None, "fs", "tp"),
            P(None, "fs", "tp"),
            P(None, "tp", None),
            P(None, "tp", None),
        ),
        out_specs=(
            P(None, None, "fs"),
            P(None, None, "fs"),
            P(None, None, "fs"),
            P("fs", "tp", None),
        ),
        check_vma=False,
    )
```

```python
import functools

import jax
import jax.numpy as jnp
from jax import lax
from jax.experimental import pallas as pl
from jax.experimental.pallas import tpu as pltpu
from jax.sharding import PartitionSpec as P

norm_eps = 1e-05
MESH = pl.DeviceIdType.MESH
BF16, F32 = jnp.bfloat16, jnp.float32
NZ, NX, NC = 8, 4, 2


ALL = NZ * NX * NC
LANES = (slice(0, 128), slice(128, 256), slice(0, 256))
HALF = (0, 0, 1)
DOWN = tuple((8 * j, 8) for j in range(8))
AHEAD = 2


def order_of_steps():
    sizes = [count / 8 for _, count in DOWN]
    own, when, y, x = [-1.0] * AHEAD, [], 0.0, 0.0
    for j, size in enumerate(sizes):
        if j >= AHEAD:
            when.append((own[j] + 0.8, 0, "F", j))
        y = max(y, own[j] + 0.8) + size / 3
        done = y + 0.8
        if j + AHEAD < len(DOWN):
            y += 2 * sizes[j + AHEAD] / 3
            own.append(y)
        x = max(x, done + 0.8) + size
        when += [(done, 1, "a", j), (done + 0.8, 2, "b", j), (x + 1.5, 3, "c", j), (x + 100, 4, "d", j)]
    return [(step, j) for _, _, step, j in sorted(when)]


def main_kernel(gate_in, up_in, down_in, gain_in, tok, ids_in, mix_in, gate_out, up_out, down_out, mixed,
                raw, gainv, idsv, mixv, gates, pg, pd, lg, ld, wg, dn, tokv, normed, hid, part, own, core_land,
                xs, x_land, zs, z_land, s1_send, s1_recv, s2_send, s2_recv, ag_send, ag_recv,
                core_send, core_recv, x_send, x_recv, z_send, z_recv, in_sem):
    f, t = lax.axis_index("fs"), lax.axis_index("tp")
    z, x, c = lax.div(f, NX * NC), lax.rem(lax.div(f, NC), NX), lax.rem(f, NC)
    mate = f + 1 - 2 * c
    right, left, far = lax.rem(t + 1, 4), lax.rem(t + 3, 4), lax.rem(t + 2, 4)

    def remote(src, dst, send, recv, device):
        return pltpu.make_async_remote_copy(
            src_ref=src, dst_ref=dst, send_sem=send, recv_sem=recv, device_id=device, device_id_type=MESH)

    def others(act):
        def some(m, carry):
            for zi in range(NZ):
                zo = (zi + 1) // 2 if zi % 2 else NZ - zi // 2
                zd = lax.rem(z + zo, NZ)
                xd = lax.rem(x + lax.rem(m + zi, NX), NX)
                cd = lax.rem(c + lax.div(m, NX), NC)
                u = zd * (NX * NC) + xd * NC + cd
                if zi == 0:
                    pl.when(m > 0)(functools.partial(act, u))
                else:
                    act(u)
            return carry

        lax.fori_loop(0, NZ, some, 0)

    def enter():
        barrier = pltpu.get_barrier_semaphore()

        def greet(device):
            pl.semaphore_signal(barrier, inc=1, device_id=device, device_id_type=MESH)

        near = [lax.rem(x + xo, NX) * NC + lax.rem(c + co, NC) for xo in (2, 1, 3, 0) for co in range(NC)]
        for zo in (4, 3, 5, 2, 6, 1, 7, 0):
            base = lax.rem(z + zo, NZ) * (NX * NC)
            for n, u in enumerate(near):
                if zo or n != 2 * NX - 2:
                    greet((base + u, t))
        for d in (2, 1, 3):
            greet((f, lax.rem(t + d, 4)))
        return barrier

    def raw_copy(i):
        return pltpu.make_async_copy((gate_in, up_in, down_in)[i], raw.at[i], in_sem.at[i])

    def small_copy(i):
        src, dst = ((gain_in, gainv), (ids_in, idsv), (mix_in, mixv))[i]
        return pltpu.make_async_copy(src, dst, in_sem.at[3 + i])

    def tok_copy(i):
        return pltpu.make_async_copy(tok.at[:, i], tokv.at[i], in_sem.at[6 + i])

    def pack(i):
        low = lax.broadcasted_iota(jnp.int32, (32, 128), 1) < 64
        square = [lax.broadcasted_iota(jnp.int32, (32, 32), axis) for axis in (0, 1)]
        spread = jnp.where(square[0] == square[1], jnp.broadcast_to(gainv[...], (32, 32)), 0.0)
        scale = jnp.sum(spread, axis=1, keepdims=True)
        raw_copy(i).wait()

        def some(q, carry):
            for j in range(8):
                a, b = (raw[i, 2 * q + e, :, 128 * j:128 * (j + 1)] for e in range(2))
                if i < 2:
                    a, b = a * scale, b * scale
                even = jnp.where(low, a, pltpu.roll(b, 64, 1)).astype(BF16)
                odd = jnp.where(low, pltpu.roll(a, 64, 1), b).astype(BF16)
                for o, v in enumerate((even, odd)):
                    if i < 2:
                        for half in range(2):
                            pg[half, q, 2 * j + o, :, 128 * i:128 * (i + 1)] = v[16 * half:16 * (half + 1)]
                    else:
                        pd[q, 2 * j + o] = v
            return carry

        lax.fori_loop(0, 4, some, 0)
        if i < 2:
            for half in range(2):
                lanes = slice(128 * i, 128 * (i + 1))
                lg[half, pl.ds(16 * t, 16), :, lanes] = pg[half, t, :, :, lanes]
        else:
            ld[pl.ds(16 * t, 16)] = pd[t]

    def place(core):
        return lax.rem(core + c + 1, NC)

    def spread_gates():
        small_copy(1).wait()
        small_copy(2).wait()
        for q in range(4):
            sides = []
            for e in (2 * q, 2 * q + 1):
                row = sum(jnp.where(idsv[k:k + 1, :] == e, mixv[k:k + 1, :], 0.0) for k in range(2))
                sides.append(jnp.broadcast_to(row, (64, 768)))
            turned = jnp.concatenate(sides, axis=0).T
            for ci in range(NC):
                for xi in range(NX):
                    for zi in range(NZ):
                        at, by = 96 * xi + 12 * zi, 96 * zi + 24 * xi + 12 * ci
                        gates[q, place(ci), at:at + 12, :] = turned[by:by + 12, :]

    def s1(k, d):
        q = lax.rem(t + d, 4)
        sems = (s1_send.at[k // 3], s1_recv.at[k], (f, q))
        if k < 3:
            return remote(pg.at[HALF[k], q, :, :, LANES[k]], lg.at[HALF[k], pl.ds(16 * t, 16), :, LANES[k]], *sems)
        return remote(pd.at[q], ld.at[pl.ds(16 * t, 16)], *sems)

    def s1_start(k):
        for d in (2, 1, 3):
            s1(k, d).start()

    def s1_all(k):
        sems = (s1_send.at[k // 3], s1_recv.at[k], (f, right))
        if k < 3:
            return remote(pg.at[HALF[k], pl.ds(0, 3), :, :, LANES[k]], pg.at[HALF[k], pl.ds(0, 3), :, :, LANES[k]], *sems)
        return remote(pd.at[pl.ds(0, 3)], pd.at[pl.ds(0, 3)], *sems)

    def s1_wait(k):
        s1_all(k).wait_recv()

    def s2_send_all(k):
        def go(u):
            sems = (s2_send.at[k // 3], s2_recv.at[k], (u, t))
            if k < 3:
                remote(lg.at[HALF[k], u, :, LANES[k]], wg.at[t, f, HALF[k], :, LANES[k]], *sems).start()
            else:
                remote(ld.at[u], dn.at[t, f], *sems).start()

        others(go)
        if k < 3:
            wg[t, f, HALF[k], :, LANES[k]] = lg[HALF[k], f, :, LANES[k]]
        else:
            dn[t, f] = ld[f]

    def s2_all(k):
        blocks = pl.ds(0, ALL - 1)
        sems = (s2_send.at[k // 3], s2_recv.at[k], (mate, t))
        if k < 3:
            return remote(lg.at[HALF[k], blocks, :, LANES[k]], wg.at[t, blocks, HALF[k], :, LANES[k]], *sems)
        return remote(ld.at[blocks], dn.at[t, blocks], *sems)

    def ag_piece(k, q, piece):
        if k < 3:
            return wg.at[q, pl.ds(32 * piece, 32), HALF[k], :, LANES[k]]
        first, count = DOWN[k - 3]
        return dn.at[q, pl.ds(first + count // 2 * piece, count // 2)]

    def ag_group(k, group):
        return 4 * k + group if k < 3 else 12 + 3 * (k - 3) + min(group, 2)

    def ag(k, slot):
        piece = (0, 1, 0, 1, 0, 1)[slot]
        to = (right, right, left, left, right, left)[slot]
        q = (t, t, t, t, left, right)[slot]
        ref = ag_piece(k, q, piece)
        return remote(ref, ref, ag_send.at[min(k, 3) // 3], ag_recv.at[ag_group(k, (0, 2, 2, 1, 3, 3)[slot])], (f, to))

    def ag_own(k):
        for slot in (0, 3, 1, 2):
            ag(k, slot).start()

    def ag_arrived(k, group):
        if group < 2:
            ref = ag_piece(k, (left, right)[group], group)
        elif k < 3:
            ref = wg.at[far, :, HALF[k], :, LANES[k]]
        else:
            ref = dn.at[pl.ds(0, 2), pl.ds(*DOWN[k - 3])]
        remote(ref, ref, ag_send.at[min(k, 3) // 3], ag_recv.at[ag_group(k, group)], (f, right)).wait_recv()

    def ag_forward(k):
        ag_arrived(k, 0)
        ag(k, 4).start()
        ag_arrived(k, 1)
        ag(k, 5).start()

    def norm(i):
        tok_copy(i).wait()

        def four(a, carry):
            v = jnp.concatenate([tokv[i, 4 * a + b].astype(F32) for b in range(4)], axis=0)
            mean = jnp.mean(v, axis=1, keepdims=True)
            v = v - mean
            var = jnp.mean(v * v, axis=1, keepdims=True)
            v = v * lax.rsqrt(var + norm_eps)
            for ci in range(NC):
                some = jnp.concatenate([v[24 * b + 12 * ci:24 * b + 12 * (ci + 1)] for b in range(4)], axis=0)
                rows = pl.ds(pl.multiple_of(96 * i + 48 * a, 16), 48)
                normed[place(ci), rows, :] = some.astype(BF16)
            return carry

        lax.fori_loop(0, NZ // 4, four, 0)

    def hidden(q):
        def some(r, carry):
            act = jnp.dot(normed[r], wg[q].reshape(2048, 256), preferred_element_type=F32)
            gate_act, up_act = act[:, :128], act[:, 128:]
            value = gate_act / (1.0 + jnp.exp(-gate_act)) * up_act * gates[q, r]
            hid[r, :, pl.ds(pl.multiple_of(q * 128, 128), 128)] = value.astype(BF16)
            return carry

        lax.fori_loop(0, NC, some, 0)

    def turn_both(q):
        for i in range(4):
            both = wg[q, 16 * i:16 * (i + 1)].reshape(512, 256).T
            for n, out in enumerate((gate_out, up_out)):
                for e in range(2):
                    out[2 * q + e, :, 512 * i:512 * (i + 1)] = both[128 * n + 64 * e:128 * n + 64 * (e + 1), :]

    def wide(j):
        return pl.ds(0, 32 * DOWN[j][1])

    def core_copy(j):
        return remote(part.at[j, :, wide(j)], core_land.at[j, :, wide(j)], core_send.at[0], core_recv.at[j], (mate, t))

    def x_start(j):
        for d in (2, 1, 3):
            xd = lax.rem(x + d, NX)
            remote(xs.at[j, xd, :, wide(j)], x_land.at[j, d - 1, :, wide(j)], x_send.at[0], x_recv.at[j],
                   (z * (NX * NC) + xd * NC + c, t)).start()

    def x_all(j):
        return remote(xs.at[j, pl.ds(0, NX - 1), :, wide(j)], x_land.at[j, :, :, wide(j)], x_send.at[0], x_recv.at[j],
                      (mate, t))

    def z_start(j):
        for d in (4, 3, 5, 2, 6, 1, 7):
            zd = lax.rem(z + d, NZ)
            remote(zs.at[j, zd, :, wide(j)], z_land.at[j, d - 1, :, wide(j)], z_send.at[0], z_recv.at[j],
                   (zd * (NX * NC) + x * NC + c, t)).start()

    def z_all(j):
        return remote(zs.at[j, pl.ds(0, NZ - 1), :, wide(j)], z_land.at[j, :, :, wide(j)], z_send.at[0], z_recv.at[j],
                      (mate, t))

    def forward(j):
        ag_forward(j + 3)
        if j + AHEAD < len(DOWN):
            ag_own(j + AHEAD + 3)

    def step_a(j):
        ag_arrived(j + 3, 2)
        first, count = DOWN[j]
        turned = [dn[q, first:first + count].reshape(32 * count, 128).T for q in range(4)]
        block = jnp.concatenate(turned, axis=0)
        total = jnp.dot(hid[...].reshape(768, 512), block, preferred_element_type=F32)
        part[j, :, wide(j)] = total[:384].astype(BF16)
        core_copy(j).start()
        own[j % 2, :, wide(j)] = total[384:]
        for q in range(4):
            for e in range(2):
                down_out[2 * q + e, :, 32 * first:32 * (first + count)] = turned[q][64 * e:64 * (e + 1), :]

    def step_b(j):
        core_copy(j).wait_recv()
        for i in range(NX):
            rows = slice(96 * i, 96 * (i + 1))
            xs[j, i, :, wide(j)] = (
                own[j % 2, rows, wide(j)] + core_land[j, rows, wide(j)].astype(F32)).astype(BF16)
        x_start(j)

    def step_c(j):
        x_all(j).wait_recv()
        total = xs[j, x, :, wide(j)].astype(F32)
        for d in range(3):
            total += x_land[j, d, :, wide(j)].astype(F32)
        for zi in range(NZ):
            zs[j, zi, :, wide(j)] = total[12 * zi:12 * (zi + 1)].astype(BF16)
        z_start(j)

    def step_d(j):
        z_all(j).wait_recv()
        total = zs[j, z, :, wide(j)].astype(F32)
        for d in range(NZ - 1):
            total += z_land[j, d, :, wide(j)].astype(F32)
        first, count = DOWN[j]
        mixed[:, 32 * first:32 * (first + count)] = total.astype(BF16)

    scope = jax.named_scope
    with scope("begin"):
        small_copy(0).start()
        raw_copy(0).start()
        barrier = enter()
        for i in (1, 2):
            raw_copy(i).start()
            small_copy(i).start()
        for i in range(NX):
            tok_copy(i).start()
        small_copy(0).wait()
    with scope("pack"):
        pack(0)
    with scope("barrier"):
        pl.semaphore_wait(barrier, ALL + 2)
        s1_start(0)
    with scope("pack_rest"):
        pack(1)
        pack(2)
        s1_start(1)
        s1_start(2)

    with scope("s1_0"):
        s1_wait(0)
        s1_start(3)
        s2_send_all(0)
    with scope("norm_0"):
        norm(0)
    with scope("s1_1"):
        s1_wait(1)
        s2_send_all(1)
    with scope("norm_1"):
        norm(1)
        norm(2)
    with scope("s1_2"):
        s1_wait(2)
        s2_send_all(2)
    with scope("norm_2"):
        norm(3)
    with scope("s2_0"):
        s2_all(0).wait_recv()
        ag_own(0)
    with scope("s1_3"):
        s1_wait(3)
        s2_send_all(3)
    with scope("gates"):
        spread_gates()
    with scope("s2_1"):
        s2_all(1).wait_recv()
        ag_own(1)
    with scope("fwd_0"):
        ag_forward(0)
    with scope("fwd_1"):
        ag_forward(1)
    with scope("s2_2"):
        s2_all(2).wait_recv()
        ag_own(2)
    with scope("hidden_t"):
        hidden(t)
    with scope("turn_t"):
        turn_both(t)
    with scope("s2_3"):
        s2_all(3).wait_recv()
        for j in range(AHEAD):
            ag_own(3 + j)
    with scope("fwd_2"):
        ag_forward(2)
    with scope("near"):
        for k in range(3):
            ag_arrived(k, 2)
    with scope("hidden_lr"):
        hidden(left)
        hidden(right)
    with scope("turn_lr"):
        turn_both(left)
        turn_both(right)
    with scope("fwd_down"):
        for j in range(AHEAD):
            ag_forward(j + 3)
    with scope("far"):
        for k in range(3):
            ag_arrived(k, 3)
        for j in range(AHEAD):
            ag_own(j + AHEAD + 3)
    with scope("hidden_far"):
        hidden(far)
    steps = dict(F=forward, a=step_a, b=step_b, c=step_c, d=step_d)
    for step, j in order_of_steps():
        with scope(f"step_{step}{j}"):
            steps[step](j)
            if step == "b" and j == len(DOWN) - 1:
                turn_both(far)

    with scope("drain"):
        def sent(ref, sem):
            remote(ref, ref, sem, s1_recv.at[0], (mate, t)).wait_send()

        sent(pg.at[:, pl.ds(0, 3)], s1_send.at[0])
        sent(pd.at[pl.ds(0, 3)], s1_send.at[1])
        sent(wg.at[0, pl.ds(0, ALL - 1)], s2_send.at[0])
        sent(dn.at[0, pl.ds(0, ALL - 1)], s2_send.at[1])
        sent(wg.at[pl.ds(0, 3)], ag_send.at[0])
        sent(dn.at[pl.ds(0, 3)], ag_send.at[1])
        if len({count for _, count in DOWN}) > 1:
            for j in range(len(DOWN)):
                sent(part.at[j, :, wide(j)], core_send.at[0])
                sent(x_land.at[j, :, :, wide(j)], x_send.at[0])
                sent(z_land.at[j, :, :, wide(j)], z_send.at[0])
        else:
            sent(part, core_send.at[0])
            sent(x_land, x_send.at[0])
            sent(z_land, z_send.at[0])


def exchange(gate, up, down, gain, tok, ids, mix):
    dma, vmem = pltpu.SemaphoreType.DMA, pltpu.VMEM
    whole = pl.BlockSpec(memory_space=pltpu.VMEM)
    serve = jax.ShapeDtypeStruct((8, 64, 2048), BF16)
    n, width = len(DOWN), 32 * max(count for _, count in DOWN)
    return pl.pallas_call(
        main_kernel,
        in_specs=[pl.BlockSpec(memory_space=pltpu.HBM)] * 7,
        out_specs=[whole] * 4,
        out_shape=(serve, serve, serve, jax.ShapeDtypeStruct((12, 2048), BF16)),
        scratch_shapes=[
            vmem((3, 8, 32, 1024), F32),
            vmem((1, 32), F32),
            vmem((2, 768), jnp.int32),
            vmem((2, 768), F32),
            vmem((4, NC, 384, 128), F32),
            vmem((2, 4, 16, 16, 256), BF16),
            vmem((4, 16, 32, 128), BF16),
            vmem((2, 64, 16, 256), BF16),
            vmem((64, 32, 128), BF16),
            vmem((4, 64, 2, 16, 256), BF16),
            vmem((4, 64, 32, 128), BF16),
            vmem((NX, NZ, 24, 2048), BF16),
            vmem((NC, 384, 2048), BF16),
            vmem((NC, 384, 512), BF16),
            vmem((n, 384, width), BF16),
            vmem((2, 384, width), F32),
            vmem((n, 384, width), BF16),
            vmem((n, NX, 96, width), BF16),
            vmem((n, NX - 1, 96, width), BF16),
            vmem((n, NZ, 12, width), BF16),
            vmem((n, NZ - 1, 12, width), BF16),
            dma((2,)), dma((4,)),
            dma((2,)), dma((4,)),
            dma((2,)), dma((12 + 3 * n,)),
            dma((1,)), dma((n,)),
            dma((1,)), dma((n,)),
            dma((1,)), dma((n,)),
            dma((10,)),
        ],
        compiler_params=pltpu.CompilerParams(
            has_side_effects=True, collective_id=0, vmem_limit_bytes=44 * 2**20),
    )(*(pltpu.with_memory_space_constraint(a, pltpu.HBM) for a in (gate, up, down, gain, tok, ids, mix)))


def copy_kernel(*refs):
    half = len(refs) // 2
    copies = []
    for src, dst in zip(refs[:half], refs[half:]):
        pieces = [slice(None)] if src.ndim == 2 else [pl.ds(i, 4) for i in range(0, src.shape[0], 4)]
        copies += [pltpu.make_async_copy(src.at[p], dst.at[p], refs[-1].at[len(copies) + n]) for n, p in enumerate(pieces)]
    for copy in copies:
        copy.start()
    for copy in copies:
        copy.wait()


def copied(arrays):
    anywhere = pl.BlockSpec(memory_space=pl.ANY)
    return pl.pallas_call(
        copy_kernel,
        in_specs=[anywhere] * len(arrays),
        out_specs=[pl.BlockSpec(memory_space=pltpu.HBM)] * len(arrays),
        out_shape=tuple(jax.ShapeDtypeStruct(a.shape, a.dtype) for a in arrays),
        scratch_shapes=[pltpu.SemaphoreType.DMA((7,))],
        compiler_params=pltpu.CompilerParams(vmem_limit_bytes=2**20),
    )(*arrays)


def local(tokens, norm_gain, gate_weight, up_weight, down_weight, expert_ids, expert_mix):
    *serve, mixed = copied(exchange(
        gate_weight, up_weight, down_weight, norm_gain[None, :], tokens.reshape(NZ, NX, 24, 2048),
        expert_ids.reshape(768, 2).T, expert_mix.reshape(768, 2).T))
    return tuple(jnp.swapaxes(out, 1, 2) for out in serve) + (mixed.reshape(12, 1, 2048),)


def solution(mesh):
    return jax.shard_map(
        local,
        mesh=mesh,
        in_specs=(
            P(None, "tp", None),
            P("fs"),
            P(None, "fs", "tp"),
            P(None, "fs", "tp"),
            P(None, "fs", "tp"),
            P(None, "tp", None),
            P(None, "tp", None),
        ),
        out_specs=(
            P(None, None, "fs"),
            P(None, None, "fs"),
            P(None, None, "fs"),
            P("fs", "tp", None),
        ),
        check_vma=False,
    )
```
